32 devices in a mesh: kv: 8 (over z, y), tp: 4 (over x, core).
Axes of the slice: x: 2, y: 2, z: 4, core: 2. Of those that a mesh axis runs over, the one named last changes fastest.
Arguments:
- query_rows: bfloat16 [16384, 1536], P('kv', 'tp'), may hold values from -6 to 6
- key_rows: bfloat16 [16384, 1536], P('kv', 'tp'), may hold values from -6 to 6
- value_rows: bfloat16 [16384, 1536], P('kv', 'tp'), may hold values from -6 to 6
- log_sums: float32 [12, 16384], P('tp', 'kv'), may hold values from 5.5 to 7.5
- cotangent: bfloat16 [16384, 1536], P('kv', 'tp'), may hold values from -24 to 24
- layer_input: bfloat16 [16384, 4096], P('kv', 'tp'), may hold values from -0.29882812 to 0.29882812
- chosen: int32 [12, 512, 12], P('tp'), may hold values from -1 to 447, as said below
Outputs:
- grad_queries: bfloat16 [16384, 1536], P('kv', 'tp')
- grad_keys: float32 [16384, 1536], P('kv', 'tp')
- grad_values: float32 [16384, 1536], P('kv', 'tp')
- grad_weight: float32 [4096, 1536], P(('tp', 'kv'))
The draws below stay inside these ranges and needn't reach their ends.
Inputs may be any that keep to these rules, and one draw needn't show every extreme that they name: `chosen`: for query block i, write j = i // 64. Every entry other than -1 names a block below j * 64; the entries of a row are distinct, the -1 entries stand last, and a row has exactly min(12, 2 * min(j, 7)) entries other than -1. For one head, the rows with the same j name at most 2 distinct blocks of any one span; for j >= 1 the span j - 1 gives exactly 2 blocks, named by every such row.
All inputs are finite; a program needn't handle non-finite values.
Results may differ from the reference program's by a relative error of at most 0.007.
Values may be sent and summed in bfloat16 or wider, within the bound.
A program may use at most 192 MiB of HBM per device.

```python
import jax
import jax.numpy as jnp
from jax import lax

D = 4096
HEADS = 12
HEAD_DIM = 128
KEY_BLOCK = 32
SEL = 12
CAP = 2
OWNERS = 7
TOKENS = 16384
BPD = 64
N_KV = 8


def draw_chosen(key, part):
    base_key = jax.random.fold_in(key, 17)
    owner_key, block_key, row_key = jax.random.split(base_key, 3)
    asking_accelerator = jnp.arange(N_KV, dtype=jnp.int32)[:, None]
    proposed_segment = jnp.arange(N_KV, dtype=jnp.int32)[None, :]
    noise_perturbation = jax.random.randint(owner_key, (HEADS, N_KV, N_KV), 0, 1 << 20, dtype=jnp.int32) * 64 + proposed_segment
    merit_increment = jnp.where(proposed_segment == asking_accelerator - 1, 3 << 27, jnp.where(proposed_segment == asking_accelerator - N_KV // 2, 2 << 27, jnp.where(proposed_segment == 0, 1 << 27, 0)))
    possessor_merit = jnp.where(proposed_segment < asking_accelerator, noise_perturbation + merit_increment, -1 - proposed_segment)
    owner_top, owner_pick = lax.top_k(possessor_merit, OWNERS)
    owner_valid = owner_top >= 0
    block_noise = jax.random.randint(block_key, (HEADS, N_KV, OWNERS, BPD), 0, 1 << 20, dtype=jnp.int32) * BPD + jnp.arange(BPD, dtype=jnp.int32)
    block_top, block_pick = lax.top_k(block_noise, CAP)
    pool_ids = (owner_pick[:, :, :, None] * BPD + block_pick).reshape(HEADS, N_KV, OWNERS * CAP)
    pool_valid = jnp.repeat(owner_valid, CAP, axis=2)
    pool_size = OWNERS * CAP
    slot_ids = jnp.arange(pool_size, dtype=jnp.int32)
    row_noise = jax.random.randint(row_key, (HEADS, N_KV, BPD, pool_size), 0, 1 << 20, dtype=jnp.int32) * pool_size + slot_ids
    row_noise = row_noise + jnp.where(slot_ids < 2 * CAP, 1 << 27, 0)
    row_score = jnp.where(pool_valid[:, :, None, :], row_noise, -1 - slot_ids)
    row_top, row_pick = lax.top_k(row_score, SEL)
    picked = jnp.take_along_axis(jnp.broadcast_to(pool_ids[:, :, None, :], row_score.shape), row_pick, axis=3)
    result = jnp.where(row_top >= 0, picked, -1)
    return result.reshape(HEADS, N_KV * BPD, SEL).astype(jnp.int32)


def block_levels(stream_key, shape, shards, smallest, high):
    level, own = 1.0, jax.random.fold_in(stream_key, 6)
    for dim, blocks in shards:
        heights = jnp.exp(jax.random.uniform(jax.random.fold_in(own, dim), (blocks,), jnp.float32, smallest / len(shards), high / len(shards)))
        level = level * jnp.repeat(heights, shape[dim] // blocks).reshape([-1 if axis == dim else 1 for axis in range(len(shape))])
    return level


def gaussian(own_key, shape, deviation, most, cuts=(), kind=jnp.bfloat16):
    entries = deviation * jax.random.normal(own_key, shape, jnp.float32)
    if cuts:
        entries = entries * block_levels(own_key, shape, cuts, -0.22, 0.18)
    return jnp.clip(entries, -most, most).astype(kind)


def setup_inputs(seed: int = 0) -> dict:
    seeds = jax.random.split(jax.random.key(seed), 8)
    return {
        "query_rows": gaussian(seeds[0], (TOKENS, HEADS * HEAD_DIM), 1.0, 6.0, ((0, 8), (1, 4))),
        "key_rows": gaussian(seeds[1], (TOKENS, HEADS * HEAD_DIM), 1.0, 6.0, ((0, 8), (1, 4))),
        "value_rows": gaussian(seeds[2], (TOKENS, HEADS * HEAD_DIM), 1.0, 6.0, ((0, 8), (1, 4))),
        "log_sums": jnp.clip(5.5 + 2.0 * jax.random.uniform(seeds[3], (HEADS, TOKENS), jnp.float32) ** block_levels(seeds[3], (HEADS, TOKENS), ((0, 4), (1, 8)), -0.2, 0.2), 5.5, 7.5),
        "cotangent": gaussian(seeds[4], (TOKENS, HEADS * HEAD_DIM), 4.0, 24.0, ((0, 8), (1, 4))),
        "layer_input": gaussian(seeds[5], (TOKENS, D), 0.05, 0.29882812, ((0, 8), (1, 4))),
        "chosen": draw_chosen(jax.random.fold_in(seeds[7], 71), 0),
    }


def head_grads(inputs):
    query_portion, key_part, value_part, output_gradient, log_sum, picked = inputs
    blocks = query_portion.shape[0] // KEY_BLOCK
    scale_factor = HEAD_DIM ** -0.5
    batch_query = query_portion.reshape(blocks, KEY_BLOCK, HEAD_DIM).astype(jnp.float32)
    key_b = key_part.reshape(blocks, KEY_BLOCK, HEAD_DIM).astype(jnp.float32)
    value_b = value_part.reshape(blocks, KEY_BLOCK, HEAD_DIM).astype(jnp.float32)
    batch_gradient = output_gradient.reshape(blocks, KEY_BLOCK, HEAD_DIM).astype(jnp.float32)
    sums_b = log_sum.reshape(blocks, KEY_BLOCK)
    usable = picked >= 0
    safe_ids = jnp.maximum(picked, 0).astype(jnp.int32)
    far_span = SEL * KEY_BLOCK
    gathered_keys = jnp.concatenate([key_b[safe_ids].reshape(blocks, far_span, HEAD_DIM), key_b], axis=1)
    gathered_values = jnp.concatenate([value_b[safe_ids].reshape(blocks, far_span, HEAD_DIM), value_b], axis=1)
    far_mask = jnp.broadcast_to(jnp.repeat(usable, KEY_BLOCK, axis=1)[:, None, :], (blocks, KEY_BLOCK, far_span))
    lower_triangular = jnp.broadcast_to(jnp.tril(jnp.ones((KEY_BLOCK, KEY_BLOCK), dtype=bool)), (blocks, KEY_BLOCK, KEY_BLOCK))
    attend_mask = jnp.concatenate([far_mask, lower_triangular], axis=2)
    attention_scores = jnp.einsum("cjw,ctw->cjt", batch_query, gathered_keys) * scale_factor
    probs = jnp.where(attend_mask, jnp.exp(attention_scores - sums_b[:, :, None]), 0.0)
    probability_gradient = jnp.einsum("cjw,ctw->cjt", batch_gradient, gathered_values)
    row_dots = jnp.sum(probs * probability_gradient, axis=2)
    score_gradient = lax.optimization_barrier((probs * (probability_gradient - row_dots[:, :, None])).astype(jnp.bfloat16))
    reduced_probabilities = lax.optimization_barrier(probs.astype(jnp.bfloat16))
    query_gradient = (scale_factor * jnp.einsum("lzs,lsa->lza", score_gradient.astype(jnp.float32), gathered_keys)).astype(jnp.bfloat16)
    full_key_gradient = scale_factor * jnp.einsum("slm,slc->smc", score_gradient.astype(jnp.float32), batch_query)
    full_value_gradient = jnp.einsum("slm,slc->smc", reduced_probabilities.astype(jnp.float32), batch_gradient)
    flat_ids = safe_ids.reshape(-1)
    empty = jnp.zeros((blocks, KEY_BLOCK, HEAD_DIM), jnp.float32)
    grad_key = full_key_gradient[:, far_span:] + empty.at[flat_ids].add(full_key_gradient[:, :far_span].reshape(blocks * SEL, KEY_BLOCK, HEAD_DIM))
    grad_value = full_value_gradient[:, far_span:] + empty.at[flat_ids].add(full_value_gradient[:, :far_span].reshape(blocks * SEL, KEY_BLOCK, HEAD_DIM))
    return query_gradient.reshape(-1, HEAD_DIM), grad_key.reshape(-1, HEAD_DIM), grad_value.reshape(-1, HEAD_DIM)


def heads_first(array):
    return array.reshape(TOKENS, HEADS, HEAD_DIM).transpose(1, 0, 2)


def heads_back(array):
    return array.transpose(1, 0, 2).reshape(TOKENS, HEADS * HEAD_DIM)


def reference(query_rows, key_rows, value_rows, log_sums, cotangent, layer_input, chosen):
    query_gradient, grad_key, grad_value = lax.map(head_grads, (heads_first(query_rows), heads_first(key_rows), heads_first(value_rows), heads_first(cotangent), log_sums, chosen))
    grad_queries = heads_back(query_gradient)
    grad_weight = jnp.dot(layer_input.T, grad_queries, preferred_element_type=jnp.float32)
    return grad_queries, heads_back(grad_key), heads_back(grad_value), grad_weight
```

```python
import functools

import jax
import jax.numpy as jnp
from jax import lax
from jax.experimental import pallas as pl
from jax.experimental.pallas import tpu as pltpu
from jax.sharding import PartitionSpec as P

HEAD_DIM = 128
KEY_BLOCK = 32
CAP = 2
SUB = 128
NEVER = -1e30
LOG2E = 1.4426950408889634

MESH = pl.DeviceIdType.MESH
NT = (((1,), (1,)), ((), ()))
NN = (((1,), (0,)), ((), ()))
TN = (((0,), (0,)), ((), ()))


def dot(a, b, dims):
    return lax.dot_general(a, b, dims, preferred_element_type=jnp.float32)


def flip(place, bit):
    return place + bit - 2 * bit * lax.rem(lax.div(place, bit), 2)


def chunk_plan(heads):
    chunks = []
    for head in range(heads):
        chunks.append((("own", head), ("came", head)))
    return chunks


def step_plan(heads):
    last = heads - 1
    plan = []
    for head in range(heads):
        plan.append(("attend", head))
        if head:
            plan.append(("product", head - 1))
    plan.append(("relay", 0))
    plan.append(("product", last))
    for head in range(1, heads):
        plan.append(("relay", head))
    return plan


class Kernel:
    def __init__(self, spans, tp_count, heads, rows, features):
        self.spans, self.tp_count, self.heads = spans, tp_count, heads
        self.rows, self.features = rows, features
        self.far_rows = (spans - 1) * CAP * KEY_BLOCK
        self.tile = 256 if self.far_rows <= 512 else SUB
        self.tiles = rows // self.tile
        self.slice = features // spans
        self.pieces = spans // 2
        self.chunks = chunk_plan(heads)
        self.plan = step_plan(heads)
        self.stages = spans.bit_length() - 1

    def scratch(self):
        spans, heads, rows = self.spans, self.heads, self.rows
        span_rows = CAP * KEY_BLOCK
        wide = heads * HEAD_DIM
        bf, f32 = jnp.bfloat16, jnp.float32
        dma = pltpu.SemaphoreType.DMA
        out = dict(
            query=pltpu.VMEM((rows, wide), bf),
            key=pltpu.VMEM((rows, wide), bf),
            value=pltpu.VMEM((rows, wide), bf),
            cot=pltpu.VMEM((rows, wide), bf),
            layer=pltpu.VMEM((rows, self.features), bf),
            turned=pltpu.VMEM((spans, 2, self.slice, rows), bf),
            far=pltpu.VMEM((heads, spans, 2, span_rows, HEAD_DIM), bf),
            back=pltpu.VMEM((heads, spans, 2, span_rows, HEAD_DIM), bf),
            acc=pltpu.VMEM((2, self.far_rows, HEAD_DIM), f32),
            dq=pltpu.VMEM((heads, rows, HEAD_DIM), bf),
            came=pltpu.VMEM((heads, rows, HEAD_DIM), bf),
            dkv=pltpu.VMEM((heads, 2, rows, HEAD_DIM), f32),
            load_sem=dma((6,)),
            store_sem=dma((heads, 3)),
            far_send=dma((heads, spans)),
            far_recv=dma((heads, spans)),
            back_send=dma((heads, spans)),
            back_recv=dma((heads, spans)),
            turn_send=dma((spans,)),
            turn_recv=dma((spans,)),
            dq_send=dma((heads, self.tiles)),
            dq_recv=dma((heads, self.tiles)),
        )
        count = len(self.chunks)
        for c, chunk in enumerate(self.chunks):
            width = HEAD_DIM * len(chunk)
            out[f"part{c}"] = pltpu.VMEM((self.pieces, 2, 2 * self.slice, width), f32)
            left = self.pieces
            for stage in range(self.stages):
                give = left if stage == 0 else left // 2
                shape = (give, 2 * self.slice, width)
                out[f"give{c}_{stage}"] = pltpu.VMEM(shape, bf)
                out[f"got{c}_{stage}"] = pltpu.VMEM(shape, bf)
                out[f"give_sem{c}_{stage}"] = dma((give,))
                out[f"got_sem{c}_{stage}"] = dma((give,))
                left = give if stage == 0 else left - give
            out[f"sum{c}"] = pltpu.VMEM((2, self.slice, width), f32)
            out[f"other{c}"] = pltpu.VMEM((self.slice, width), f32)
        out["sum_send"] = dma((count,))
        out["sum_recv"] = dma((count,))
        return out

    def body(self, names, *refs):
        fixed = (
            "bias", "picked", "query_in", "key_in", "value_in", "cot_in", "layer_in", "dq_out", "dk_out", "dv_out", "home", "weight",
        )
        for name, ref in zip(fixed + names, refs, strict=True):
            setattr(self, name, ref)
        self.me = lax.axis_index("kv")
        self.tp = lax.axis_index("tp")
        self.side = self.tp_count // 2
        self.start()
        for head in range(self.heads):
            self.send_far(head)
        self.turn()
        for kind, index in self.plan:
            getattr(self, kind)(index)
        self.finish()


    def load(self, which):
        pairs = (
            (self.key_in, self.key),
            (self.value_in, self.value),
            (self.query_in, self.query),
            (self.cot_in, self.cot),
            (self.layer_in, self.layer),
        )
        src, dst = pairs[which]
        return pltpu.make_async_copy(src, dst, self.load_sem.at[which])

    def remote(self, src, dst, send, recv, **to):
        return pltpu.make_async_remote_copy(
            src_ref=src, dst_ref=dst, send_sem=send, recv_sem=recv,
            device_id=to, device_id_type=MESH,
        )

    def far_copy(self, head, to, sender):
        return self.remote(
            self.picked.at[to, head], self.far.at[head, sender],
            self.far_send.at[head, to], self.far_recv.at[head, sender], kv=to,
        )

    def back_copy(self, head, to, sender):
        return self.remote(
            self.back.at[head, to], self.home.at[sender, head],
            self.back_send.at[head, to], self.back_recv.at[head, sender], kv=to,
        )

    def turn_copy(self, place):
        return self.remote(
            self.turned.at[place, 0], self.turned.at[place, 1],
            self.turn_send.at[place], self.turn_recv.at[place], tp=flip(self.tp, 1),
        )

    def dq_copy(self, head, tile):
        rows = pl.ds(pl.multiple_of(tile * self.tile, self.tile), self.tile)
        return self.remote(
            self.dq.at[head, rows], self.came.at[head, rows],
            self.dq_send.at[head, tile], self.dq_recv.at[head, tile],
            tp=flip(self.tp, self.side),
        )

    def give_copy(self, c, stage, slot):
        return self.remote(
            getattr(self, f"give{c}_{stage}").at[slot],
            getattr(self, f"got{c}_{stage}").at[slot],
            getattr(self, f"give_sem{c}_{stage}").at[slot],
            getattr(self, f"got_sem{c}_{stage}").at[slot],
            kv=flip(self.me, 2**stage),
        )

    def sum_copy(self, c):
        return self.remote(
            getattr(self, f"sum{c}").at[1], getattr(self, f"other{c}"),
            self.sum_send.at[c], self.sum_recv.at[c], tp=flip(self.tp, 1),
        )

    def result_copies(self, head):
        columns = pl.ds(head * HEAD_DIM, HEAD_DIM)
        pairs = (
            (self.dq.at[head], self.dq_out),
            (self.dkv.at[head, 0], self.dk_out),
            (self.dkv.at[head, 1], self.dv_out),
        )
        return [
            pltpu.make_async_copy(src, dst.at[:, columns], self.store_sem.at[head, i])
            for i, (src, dst) in enumerate(pairs)
        ]


    def start(self):
        for which in range(5):
            self.load(which).start()
        barrier = pltpu.get_barrier_semaphore()

        def greet(step, carry):
            to = lax.rem(self.me + step, self.spans)
            pl.semaphore_signal(barrier, inc=1, device_id={"kv": to}, device_id_type=MESH)
            return carry

        lax.fori_loop(1, self.spans, greet, 0)
        for bit in (1, self.side):
            pl.semaphore_signal(
                barrier, inc=1, device_id={"tp": flip(self.tp, bit)}, device_id_type=MESH
            )

        def blank(span, carry):
            for head in range(self.heads):
                self.far[head, span] = jnp.zeros(self.far.shape[2:], jnp.bfloat16)
            return carry

        lax.fori_loop(self.me, self.spans, blank, 0)
        pl.semaphore_wait(barrier, self.spans + 1)

    def send_far(self, head):
        def send(to, carry):
            self.far_copy(head, to, self.me).start()
            return carry

        lax.fori_loop(self.me + 1, self.spans, send, 0)

    def turn(self):
        self.load(4).wait()
        group = HEAD_DIM // self.slice
        step_rows = 512

        def one(g, carry):
            columns = pl.ds(pl.multiple_of(g * HEAD_DIM, HEAD_DIM), HEAD_DIM)
            for at in range(0, self.rows, step_rows):
                block = self.layer[at : at + step_rows, columns].T
                for j in range(group):
                    self.turned[g * group + j, 0, :, at : at + step_rows] = block[
                        j * self.slice : (j + 1) * self.slice
                    ]

            @pl.when(g > 0)
            def _():
                for j in range(group):
                    self.turn_copy((g - 1) * group + j).start()

            return carry

        last = self.features // HEAD_DIM
        lax.fori_loop(0, last, one, 0)
        for which in range(4):
            self.load(which).wait()
        for j in range(group):
            self.turn_copy((last - 1) * group + j).start()

    def attend(self, head):
        def arrived(span, carry):
            self.far_copy(head, self.me, span).wait_recv()
            return carry

        lax.fori_loop(0, self.me, arrived, 0)
        lax.fori_loop(0, self.tiles, functools.partial(self.attend_tile, head), 0)
        self.dq_copy(head, self.tiles - 1).start()
        for copy in self.result_copies(head):
            copy.start()
        scale = HEAD_DIM ** (-0.5)
        spans = self.spans
        shape = (spans - 1, CAP * KEY_BLOCK, HEAD_DIM)
        self.back[head, : spans - 1, 0] = (scale * self.acc[0]).astype(jnp.bfloat16).reshape(shape)
        self.back[head, : spans - 1, 1] = self.acc[1].astype(jnp.bfloat16).reshape(shape)

        def send(to, carry):
            self.back_copy(head, to, self.me).start()
            return carry

        lax.fori_loop(0, self.me, send, 0)

    def attend_tile(self, head, step, carry):
        tile, spans, far_rows = self.tile, self.spans, self.far_rows
        scale = HEAD_DIM ** (-0.5)
        columns = slice(head * HEAD_DIM, (head + 1) * HEAD_DIM)
        rows = pl.ds(pl.multiple_of(step * tile, tile), tile)
        query = self.query[rows, columns]
        key = self.key[rows, columns]
        value = self.value[rows, columns]
        cot = self.cot[rows, columns]
        far_k = self.far[head, : spans - 1, 0].reshape(far_rows, HEAD_DIM)
        far_v = self.far[head, : spans - 1, 1].reshape(far_rows, HEAD_DIM)
        far_bias = self.bias[head, : (spans - 1) * CAP, rows]
        sums = self.bias[head, spans * CAP :, rows]
        far_bias = jnp.broadcast_to(
            far_bias[:, None, :], ((spans - 1) * CAP, KEY_BLOCK, tile)
        ).reshape(far_rows, tile)
        j = lax.broadcasted_iota(jnp.int32, (SUB, tile), 0)
        t = lax.broadcasted_iota(jnp.int32, (SUB, tile), 1) % SUB
        own_ok = (j // KEY_BLOCK == t // KEY_BLOCK) & (j <= t)
        own_bias = jnp.where(own_ok, 0.0, NEVER) + sums[0:1]

        parts = [slice(at, at + SUB) for at in range(0, tile, SUB)]
        own_s = jnp.concatenate([dot(key[r, :], query[r, :], NT) for r in parts], axis=1)
        own_g = jnp.concatenate([dot(value[r, :], cot[r, :], NT) for r in parts], axis=1)
        far_s = dot(far_k, query, NT)
        far_g = dot(far_v, cot, NT)
        far_p = jnp.exp2(far_s * (scale * LOG2E) + far_bias)
        own_p = jnp.exp2(own_s * (scale * LOG2E) + own_bias)
        row_dots = jnp.sum(far_p * far_g, axis=0, keepdims=True) + jnp.sum(
            own_p * own_g, axis=0, keepdims=True
        )
        far_d = (far_p * (far_g - row_dots)).astype(jnp.bfloat16)
        own_d = (own_p * (own_g - row_dots)).astype(jnp.bfloat16)
        far_low = far_p.astype(jnp.bfloat16)
        own_low = own_p.astype(jnp.bfloat16)

        far_q = dot(far_d, far_k, TN)
        for r in parts:
            dq = far_q[r, :] + dot(own_d[:, r], key[r, :], TN)
            here = pl.ds(pl.multiple_of(step * tile + r.start, SUB), SUB)
            self.dq[head, here, :] = (scale * dq).astype(jnp.bfloat16)
            self.dkv[head, 0, here, :] = scale * dot(own_d[:, r], query[r, :], NN)
            self.dkv[head, 1, here, :] = dot(own_low[:, r], cot[r, :], NN)
        step_k = dot(far_d, query, NN)
        step_v = dot(far_low, cot, NN)

        @pl.when(step == 0)
        def _():
            self.acc[0] = step_k
            self.acc[1] = step_v

        @pl.when(step > 0)
        def _():
            self.acc[0] += step_k
            self.acc[1] += step_v
            self.dq_copy(head, step - 1).start()

        return carry

    def source(self, kind, head):
        return (self.dq if kind == "own" else self.came)[head]

    def place_of(self, slot):
        left = self.pieces - 1 - slot
        place = self.me
        for bit in range(1, self.stages):
            on = lax.rem(lax.div(left, 2 ** (self.stages - 1 - bit)), 2)
            place = place + on * (flip(self.me, 2**bit) - self.me)
        return place

    def product(self, c):
        chunk = self.chunks[c]
        part = getattr(self, f"part{c}")
        give = getattr(self, f"give{c}_0")
        for kind, head in chunk:
            if kind == "came":

                def arrived(tile, carry, head=head):
                    self.dq_copy(head, tile).wait_recv()
                    return carry

                lax.fori_loop(0, self.tiles, arrived, 0)
        if c == 0:

            def turned(place, carry):
                self.turn_copy(place).wait_recv()
                return carry

            lax.fori_loop(0, self.spans, turned, 0)
        bit = lax.rem(self.me, 2)

        def one(slot, carry):
            pair = lax.div(self.place_of(slot), 2) * 2
            left = self.turned[pl.ds(pair, 2)].reshape(4 * self.slice, self.rows)
            right = jnp.concatenate([self.source(*s) for s in chunk], axis=1)
            part[slot] = dot(left, right, NN).reshape(part.shape[1:])
            give[slot] = part[slot, 1 - bit].astype(jnp.bfloat16)
            self.give_copy(c, 0, slot).start()
            return carry

        lax.fori_loop(0, self.pieces, one, 0)

    def relay(self, c):
        part = getattr(self, f"part{c}")
        bit = lax.rem(self.me, 2)
        low, ranges = 0, []
        for stage in range(1, self.stages):
            half = (self.pieces - low) // 2
            ranges.append((stage, low, half))
            low += half

        def total(slot):
            self.give_copy(c, 0, slot).wait_recv()
            value = part[slot, bit] + getattr(self, f"got{c}_0")[slot].astype(jnp.float32)
            for stage, first, half in ranges:
                if slot >= first + half:
                    at = slot - half - first
                    self.give_copy(c, stage, at).wait_recv()
                    got = getattr(self, f"got{c}_{stage}")
                    value = value + got[at].astype(jnp.float32)
                else:
                    break
            return value

        for stage, first, half in ranges:
            for slot in range(first, first + half):
                getattr(self, f"give{c}_{stage}")[slot - first] = total(slot).astype(jnp.bfloat16)
                self.give_copy(c, stage, slot - first).start()
        final = getattr(self, f"sum{c}")
        final[...] = total(self.pieces - 1).reshape(final.shape)
        self.sum_copy(c).start()
        for at, (kind, head) in enumerate(self.chunks[c]):
            self.put(self.tp, kind, head, final[0, :, at * HEAD_DIM : (at + 1) * HEAD_DIM])

    def put(self, tp, kind, head, block):
        if kind == "came":
            tp = flip(tp, self.side)
        column = pl.multiple_of((tp * self.heads + head) * HEAD_DIM, HEAD_DIM)
        self.weight[:, pl.ds(column, HEAD_DIM)] = block

    def finish(self):
        for c, chunk in enumerate(self.chunks):
            self.sum_copy(c).wait_recv()
            other = getattr(self, f"other{c}")
            for at, (kind, head) in enumerate(chunk):
                self.put(
                    flip(self.tp, 1), kind, head, other[:, at * HEAD_DIM : (at + 1) * HEAD_DIM]
                )
            self.sum_copy(c).wait_send()
            for stage in range(self.stages):
                for slot in range(getattr(self, f"give{c}_{stage}").shape[0]):
                    self.give_copy(c, stage, slot).wait_send()

        def turned(place, carry):
            self.turn_copy(place).wait_send()
            return carry

        lax.fori_loop(0, self.spans, turned, 0)
        for head in range(self.heads):

            def later(span, carry, head=head):
                self.far_copy(head, span, self.me).wait_send()
                self.back_copy(head, self.me, span).wait_recv()
                return carry

            lax.fori_loop(self.me + 1, self.spans, later, 0)

            def earlier(span, carry, head=head):
                self.back_copy(head, span, self.me).wait_send()
                return carry

            lax.fori_loop(0, self.me, earlier, 0)

            def sent(tile, carry, head=head):
                self.dq_copy(head, tile).wait_send()
                return carry

            lax.fori_loop(0, self.tiles, sent, 0)
            for copy in self.result_copies(head):
                copy.wait()


def whole_step(bias, picked, query, key, value, cot, layer, tp_count):
    spans, heads = picked.shape[:2]
    rows = query.shape[0]
    plan = Kernel(spans, tp_count, heads, rows, layer.shape[1])
    scratch = plan.scratch()
    names = tuple(scratch)
    vmem = pl.BlockSpec(memory_space=pltpu.VMEM)
    hbm = pl.BlockSpec(memory_space=pl.ANY)
    wide = heads * HEAD_DIM
    return pl.pallas_call(
        functools.partial(plan.body, names),
        out_shape=(
            jax.ShapeDtypeStruct((rows, wide), jnp.bfloat16),
            jax.ShapeDtypeStruct((rows, wide), jnp.float32),
            jax.ShapeDtypeStruct((rows, wide), jnp.float32),
            jax.ShapeDtypeStruct((spans, heads, 2, CAP * KEY_BLOCK, HEAD_DIM), jnp.bfloat16),
            jax.ShapeDtypeStruct((plan.slice, tp_count * wide), jnp.float32),
        ),
        in_specs=[vmem] + [hbm] * 6,
        out_specs=(hbm, hbm, hbm, hbm, vmem),
        scratch_shapes=list(scratch.values()),
        compiler_params=pltpu.CompilerParams(
            collective_id=0, has_side_effects=True, vmem_limit_bytes=67043328
        ),
        name="whole_step",
    )(bias, picked, query, key, value, cot, layer)


def prepare_body(chosen, sums, key_in, value_in, ids, picked, bias, key, value, found, marks, sem, mark_sem):
    loads = [
        pltpu.make_async_copy(src, dst, sem.at[i])
        for i, (src, dst) in enumerate(((key_in, key), (value_in, value)))
    ]
    for load in loads:
        load.start()
    spans, heads = picked.shape[:2]
    rows = sums.shape[1]
    blocks = rows // KEY_BLOCK
    entries = chosen.shape[2]
    first = lax.axis_index("kv") * blocks
    for head in range(heads):
        lists = chosen[head] - first
        mine = (lists >= 0) & (lists < blocks)
        low = jnp.where(mine, lists, blocks).reshape(spans, blocks, entries)
        high = jnp.where(mine, lists, 0).reshape(spans, blocks, entries)
        low = jnp.min(jnp.min(low, axis=1), axis=1, keepdims=True)
        high = jnp.max(jnp.max(high, axis=1), axis=1, keepdims=True)
        low = jnp.where(low == blocks, 0, low)
        lane = lax.broadcasted_iota(jnp.int32, (spans, 128), 1)
        found[head] = jnp.where(lane == 0, low, high)
    copy = pltpu.make_async_copy(found, marks, mark_sem)
    copy.start()

    none = spans * blocks
    row = lax.broadcasted_iota(jnp.int32, (blocks, rows), 0)
    spread = jnp.where(
        lax.broadcasted_iota(jnp.int32, (blocks, rows), 1) // KEY_BLOCK == row, 1.0, 0.0
    ).astype(jnp.bfloat16)
    for head in range(heads):
        own = chosen[head, pl.ds(pl.multiple_of(first, blocks), blocks), :]
        lane = lax.broadcasted_iota(jnp.int32, (1, spans * CAP), 1)
        wanted = jnp.full((1, spans * CAP), -2, jnp.int32)
        for span in range(spans):
            inside = (own >= span * blocks) & (own < (span + 1) * blocks)
            low = jnp.min(jnp.where(inside, own, none), axis=0, keepdims=True)
            low = jnp.min(low, axis=1, keepdims=True)
            high = jnp.max(jnp.where(inside, own, -2), axis=0, keepdims=True)
            high = jnp.max(high, axis=1, keepdims=True)
            high = jnp.where(high == low, -2, high)
            wanted = jnp.where(lane == span * CAP, low, wanted)
            wanted = jnp.where(lane == span * CAP + 1, high, wanted)
        hit = own[:, 0:1] == wanted
        for entry in range(1, entries):
            hit = hit | (own[:, entry : entry + 1] == wanted)
        hit = jnp.where(hit, 1.0, 0.0).astype(jnp.bfloat16)
        used = dot(hit, spread, TN)
        minus = sums[head : head + 1, :] * -LOG2E
        bias[head, : spans * CAP, :] = jnp.where(used > 0.5, minus, NEVER)
        bias[head, spans * CAP :, :] = jnp.broadcast_to(minus, (8, rows))

    copy.wait()
    for load in loads:
        load.wait()

    def one(span, carry):
        for head in range(heads):
            columns = slice(head * HEAD_DIM, (head + 1) * HEAD_DIM)
            for slot in range(CAP):
                block = marks[head, span, slot]
                ids[slot, head * spans + span] = block
                at = pl.ds(pl.multiple_of(block * KEY_BLOCK, KEY_BLOCK), KEY_BLOCK)
                to = slice(slot * KEY_BLOCK, (slot + 1) * KEY_BLOCK)
                picked[span, head, 0, to, :] = key[at, columns]
                picked[span, head, 1, to, :] = value[at, columns]
        return carry

    lax.fori_loop(0, spans, one, 0)


def prepare(chosen, sums, key, value, spans):
    heads, rows = sums.shape
    vmem = pl.BlockSpec(memory_space=pltpu.VMEM)
    smem = pl.BlockSpec(memory_space=pltpu.SMEM)
    hbm = pl.BlockSpec(memory_space=pl.ANY)
    return pl.pallas_call(
        prepare_body,
        out_shape=(
            jax.ShapeDtypeStruct((CAP, heads * spans), jnp.int32),
            jax.ShapeDtypeStruct((spans, heads, 2, CAP * KEY_BLOCK, HEAD_DIM), jnp.bfloat16),
            jax.ShapeDtypeStruct((heads, spans * CAP + 8, rows), jnp.float32),
        ),
        in_specs=[vmem, vmem, hbm, hbm],
        out_specs=(smem, vmem, vmem),
        scratch_shapes=[
            pltpu.VMEM(key.shape, key.dtype),
            pltpu.VMEM(value.shape, value.dtype),
            pltpu.VMEM((heads, spans, 128), jnp.int32),
            pltpu.SMEM((heads, spans, 128), jnp.int32),
            pltpu.SemaphoreType.DMA((2,)),
            pltpu.SemaphoreType.DMA,
        ],
        name="prepare_blocks",
    )(chosen, sums, key, value)


def land_body(ids_ref, own_k, own_v, home, out_k, out_v):
    spans = home.shape[0]
    head = pl.program_id(0)
    out_k[...] = own_k[...]
    out_v[...] = own_v[...]

    def one(span, carry):
        for slot in range(CAP):
            start = pl.multiple_of(ids_ref[slot, head * spans + span] * KEY_BLOCK, KEY_BLOCK)
            rows = pl.ds(start, KEY_BLOCK)
            at = slice(slot * KEY_BLOCK, (slot + 1) * KEY_BLOCK)
            out_k[rows, :] += home[span, 0, 0, at, :].astype(jnp.float32)
            out_v[rows, :] += home[span, 0, 1, at, :].astype(jnp.float32)
        return carry

    lax.fori_loop(lax.axis_index("kv") + 1, spans, one, 0)


def land(ids, own_k, own_v, home):
    spans, heads = home.shape[:2]
    rows = own_k.shape[0]
    whole = jax.ShapeDtypeStruct((rows, heads * HEAD_DIM), jnp.float32)
    column = pl.BlockSpec((rows, HEAD_DIM), lambda h: (0, h))
    return pl.pallas_call(
        land_body,
        grid=(heads,),
        out_shape=(whole, whole),
        in_specs=[
            pl.BlockSpec(memory_space=pltpu.SMEM),
            column,
            column,
            pl.BlockSpec((spans, 1) + home.shape[2:], lambda h: (0, h, 0, 0, 0)),
        ],
        out_specs=(column, column),
        name="land_blocks",
    )(ids, own_k, own_v, home)


def local(query_rows, key_rows, value_rows, log_sums, cotangent, layer_input, chosen):
    kv_count = lax.axis_size("kv")
    tp_count = lax.axis_size("tp")
    ids, picked, bias = prepare(chosen, log_sums, key_rows, value_rows, kv_count)
    dq, own_k, own_v, home, weight = whole_step(
        bias, picked, query_rows, key_rows, value_rows, cotangent, layer_input, tp_count
    )
    grad_keys, grad_values = land(ids, own_k, own_v, home)
    return dq, grad_keys, grad_values, weight


def solution(mesh):
    placed = (
        P("kv", "tp"),
        P("kv", "tp"),
        P("kv", "tp"),
        P("tp", "kv"),
        P("kv", "tp"),
        P("kv", "tp"),
        P("tp", None, None),
    )
    return jax.shard_map(
        local,
        mesh=mesh,
        in_specs=placed,
        out_specs=(P("kv", "tp"), P("kv", "tp"), P("kv", "tp"), P(("tp", "kv"), None)),
        check_vma=False,
    )
```

```python
import functools

import jax
import jax.numpy as jnp
from jax import lax
from jax.experimental import pallas as pl
from jax.experimental.pallas import tpu as pltpu
from jax.sharding import PartitionSpec as P

HEAD_DIM = 128
KEY_BLOCK = 32
CAP = 2
SUB = 128
NEVER = -1e30
LOG2E = 1.4426950408889634

MESH = pl.DeviceIdType.MESH
NT = (((1,), (1,)), ((), ()))
NN = (((1,), (0,)), ((), ()))
TN = (((0,), (0,)), ((), ()))


def dot(a, b, dims):
    return lax.dot_general(a, b, dims, preferred_element_type=jnp.float32)


def flip(place, bit):
    return place + bit - 2 * bit * lax.rem(lax.div(place, bit), 2)


def chunk_plan(heads):
    own = [("own", head) for head in range(heads)]
    came = [("came", head) for head in range(heads)]
    return [[one] for one in own[:-1]] + [[own[-1], came[0]]] + [[one] for one in came[1:]]


def step_plan(heads):
    plan = []
    for head in range(heads):
        plan += [("attend", head), ("product", head), ("send_home", head)]
        if head:
            plan.append(("first", head - 1))
    plan += [("rest", chunk) for chunk in range(heads - 2)]
    last = 2 * heads - 2
    for chunk in range(heads, last + 1):
        plan += [("product", chunk), ("first", chunk - 1)]
        if chunk == heads:
            plan.append(("rest", heads - 2))
            plan += [("settle", early) for early in range(heads - 1)]
        else:
            plan.append(("settle", chunk - 2))
        plan.append(("rest", chunk - 1))
    return plan + [("first", last), ("settle", last - 1), ("rest", last), ("settle", last)]


class Kernel:
    def __init__(self, spans, tp_count, heads, rows, features):
        self.spans, self.tp_count, self.heads = spans, tp_count, heads
        self.rows, self.features = rows, features
        self.far_rows = (spans - 1) * CAP * KEY_BLOCK
        self.tile = 1024 if self.far_rows <= 512 else 256
        self.tiles = rows // self.tile
        self.slice = features // spans
        self.pieces = spans // 2
        self.chunks = chunk_plan(heads)
        self.plan = step_plan(heads)
        self.stages = spans.bit_length() - 1

    def scratch(self):
        spans, heads, rows = self.spans, self.heads, self.rows
        span_rows = CAP * KEY_BLOCK
        wide = heads * HEAD_DIM
        bf, f32 = jnp.bfloat16, jnp.float32
        dma = pltpu.SemaphoreType.DMA
        out = dict(
            query=pltpu.VMEM((rows, wide), bf),
            key=pltpu.VMEM((rows, wide), bf),
            value=pltpu.VMEM((rows, wide), bf),
            cot=pltpu.VMEM((rows, wide), bf),
            layer=pltpu.VMEM((rows, self.features), bf),
            turned=pltpu.VMEM((spans, 2, self.slice, rows), bf),
            far=pltpu.VMEM((heads, spans, 2, span_rows, HEAD_DIM), bf),
            back=pltpu.VMEM((heads, spans, 2, span_rows, HEAD_DIM), bf),
            acc=pltpu.VMEM((2, self.far_rows, HEAD_DIM), f32),
            key_turned=pltpu.VMEM((HEAD_DIM, self.far_rows), bf),
            bias=pltpu.VMEM((heads, spans * CAP + 8, rows), f32),
            dq=pltpu.VMEM((heads, rows, HEAD_DIM), bf),
            came=pltpu.VMEM((heads, rows, HEAD_DIM), bf),
            dkv=pltpu.VMEM((heads, 2, rows, HEAD_DIM), f32),
            load_sem=dma((6,)),
            store_sem=dma((heads, 2)),
            far_send=dma((heads, spans)),
            far_recv=dma((heads, spans)),
            back_send=dma((heads, spans)),
            back_recv=dma((heads, spans)),
            turn_send=dma((spans,)),
            turn_recv=dma((spans,)),
            dq_send=dma((heads, self.tiles)),
            dq_recv=dma((heads, self.tiles)),
        )
        count = len(self.chunks)
        for c, chunk in enumerate(self.chunks):
            width = HEAD_DIM * len(chunk)
            out[f"part{c}"] = pltpu.VMEM((self.pieces, 2, 2 * self.slice, width), f32)
            left = self.pieces
            for stage in range(self.stages):
                give = left if stage == 0 else left // 2
                shape = (give, 2 * self.slice, width)
                out[f"give{c}_{stage}"] = pltpu.VMEM(shape, bf)
                out[f"got{c}_{stage}"] = pltpu.VMEM(shape, bf)
                out[f"give_sem{c}_{stage}"] = dma((give,))
                out[f"got_sem{c}_{stage}"] = dma((give,))
                left = give if stage == 0 else left - give
            out[f"sum{c}"] = pltpu.VMEM((2, self.slice, width), f32)
            out[f"other{c}"] = pltpu.VMEM((self.slice, width), f32)
        out["sum_send"] = dma((count,))
        out["sum_recv"] = dma((count,))
        return out

    def body(self, names, *refs):
        fixed = (
            "chosen", "sums", "picked", "query_in", "key_in", "value_in", "cot_in", "layer_in", "dq_out", "own", "home", "weight",
        )
        for name, ref in zip(fixed + names, refs, strict=True):
            setattr(self, name, ref)
        self.me = lax.axis_index("kv")
        self.tp = lax.axis_index("tp")
        self.side = self.tp_count // 2
        self.start()
        for head in range(self.heads):
            self.send_far(head)
        self.turn()
        self.allow()
        for kind, index in self.plan:
            getattr(self, kind)(index)
        self.finish()


    def load(self, which):
        pairs = (
            (self.key_in, self.key),
            (self.value_in, self.value),
            (self.query_in, self.query),
            (self.cot_in, self.cot),
            (self.layer_in, self.layer),
        )
        src, dst = pairs[which]
        return pltpu.make_async_copy(src, dst, self.load_sem.at[which])

    def remote(self, src, dst, send, recv, **to):
        return pltpu.make_async_remote_copy(
            src_ref=src, dst_ref=dst, send_sem=send, recv_sem=recv,
            device_id=to, device_id_type=MESH,
        )

    def far_copy(self, head, to, sender):
        return self.remote(
            self.picked.at[to, head], self.far.at[head, sender],
            self.far_send.at[head, to], self.far_recv.at[head, sender], kv=to,
        )

    def back_copy(self, head, to, sender):
        return self.remote(
            self.back.at[head, to], self.home.at[sender, head],
            self.back_send.at[head, to], self.back_recv.at[head, sender], kv=to,
        )

    def turn_copy(self, place):
        return self.remote(
            self.turned.at[place, 0], self.turned.at[place, 1],
            self.turn_send.at[place], self.turn_recv.at[place], tp=flip(self.tp, 1),
        )

    def dq_copy(self, head, tile):
        rows = pl.ds(pl.multiple_of(tile * self.tile, self.tile), self.tile)
        return self.remote(
            self.dq.at[head, rows], self.came.at[head, rows],
            self.dq_send.at[head, tile], self.dq_recv.at[head, tile],
            tp=flip(self.tp, self.side),
        )

    def give_copy(self, c, stage, slot):
        return self.remote(
            getattr(self, f"give{c}_{stage}").at[slot],
            getattr(self, f"got{c}_{stage}").at[slot],
            getattr(self, f"give_sem{c}_{stage}").at[slot],
            getattr(self, f"got_sem{c}_{stage}").at[slot],
            kv=flip(self.me, 2**stage),
        )

    def sum_copy(self, c):
        return self.remote(
            getattr(self, f"sum{c}").at[1], getattr(self, f"other{c}"),
            self.sum_send.at[c], self.sum_recv.at[c], tp=flip(self.tp, 1),
        )

    def result_copy(self, head, which):
        columns = pl.ds(head * HEAD_DIM, HEAD_DIM)
        src, dst = (
            (self.dq.at[head], self.dq_out.at[:, columns]),
            (self.dkv.at[head], self.own.at[head]),
        )[which]
        return pltpu.make_async_copy(src, dst, self.store_sem.at[head, which])


    def start(self):
        for which in range(5):
            self.load(which).start()
        barrier = pltpu.get_barrier_semaphore()

        def greet(step, carry):
            to = lax.rem(self.me + step, self.spans)
            pl.semaphore_signal(barrier, inc=1, device_id={"kv": to}, device_id_type=MESH)
            return carry

        lax.fori_loop(1, self.spans, greet, 0)
        for bit in (1, self.side):
            pl.semaphore_signal(
                barrier, inc=1, device_id={"tp": flip(self.tp, bit)}, device_id_type=MESH
            )

        def blank(span, carry):
            for head in range(self.heads):
                self.far[head, span] = jnp.zeros(self.far.shape[2:], jnp.bfloat16)
            return carry

        lax.fori_loop(self.me, self.spans, blank, 0)
        pl.semaphore_wait(barrier, self.spans + 1)

    def send_far(self, head):
        def send(step, carry):
            self.far_copy(head, self.spans - 1 - step, self.me).start()
            return carry

        lax.fori_loop(0, self.spans - 1 - self.me, send, 0)

    def allow(self):
        spans, rows, heads = self.spans, self.rows, self.heads
        blocks = rows // KEY_BLOCK
        entries = self.chosen.shape[1]
        first = self.me * blocks
        group = lax.div(first, 128) * 128
        shift = first - group
        row = lax.broadcasted_iota(jnp.int32, (128, rows), 0) - shift
        of = lax.broadcasted_iota(jnp.int32, (128, rows), 1) // KEY_BLOCK
        spread = jnp.where(row == of, 1.0, 0.0).astype(jnp.bfloat16)
        wide = (spans * CAP, 128)
        slot = lax.broadcasted_iota(jnp.int32, wide, 0)
        base = slot // CAP * blocks
        lane = lax.broadcasted_iota(jnp.int32, (1, 128), 1)
        here = (lane >= shift) & (lane < shift + blocks)
        for head in range(heads):
            at = pl.ds(pl.multiple_of(group, 128), 128)
            own = [jnp.where(here, self.chosen[head, e : e + 1, at], -1) for e in range(entries)]
            low = jnp.full(wide, spans * blocks, jnp.int32)
            high = jnp.full(wide, -2, jnp.int32)
            for entry in own:
                inside = (entry >= base) & (entry < base + blocks)
                low = jnp.minimum(low, jnp.where(inside, entry, spans * blocks))
                high = jnp.maximum(high, jnp.where(inside, entry, -2))
            low = jnp.min(low, axis=1, keepdims=True)
            high = jnp.max(high, axis=1, keepdims=True)
            high = jnp.where(high == low, -2, high)
            wanted = jnp.where(slot % CAP == 0, low, high)
            hit = own[0] == wanted
            for entry in own[1:]:
                hit = hit | (entry == wanted)
            hits = jnp.where(hit, 1.0, 0.0).astype(jnp.bfloat16)
            used = dot(hits, spread, NN)
            minus = self.sums[head : head + 1, :] * -LOG2E
            self.bias[head, : spans * CAP, :] = jnp.where(used > 0.5, minus, NEVER)
            self.bias[head, spans * CAP :, :] = jnp.broadcast_to(minus, (8, rows))

    def turn(self):
        self.load(4).wait()
        group = HEAD_DIM // self.slice
        step_rows = 512

        def one(g, carry):
            columns = pl.ds(pl.multiple_of(g * HEAD_DIM, HEAD_DIM), HEAD_DIM)
            for at in range(0, self.rows, step_rows):
                block = self.layer[at : at + step_rows, columns].T
                for j in range(group):
                    self.turned[g * group + j, 0, :, at : at + step_rows] = block[
                        j * self.slice : (j + 1) * self.slice
                    ]

            @pl.when(g > 0)
            def _():
                for j in range(group):
                    self.turn_copy((g - 1) * group + j).start()

            return carry

        last = self.features // HEAD_DIM
        lax.fori_loop(0, last, one, 0)
        for which in range(4):
            self.load(which).wait()
        for j in range(group):
            self.turn_copy((last - 1) * group + j).start()

    def attend(self, head):
        def arrived(span, carry):
            self.far_copy(head, self.me, span).wait_recv()
            return carry

        lax.fori_loop(0, self.me, arrived, 0)
        far_k = self.far[head, : self.spans - 1, 0].reshape(self.far_rows, HEAD_DIM)
        self.key_turned[...] = far_k.T
        self.acc[...] = jnp.zeros_like(self.acc)
        lax.fori_loop(0, self.tiles, functools.partial(self.attend_tile, head), 0)
        self.result_copy(head, 0).start()
        self.result_copy(head, 1).start()
        scale = HEAD_DIM ** (-0.5)
        spans = self.spans
        shape = (spans - 1, CAP * KEY_BLOCK, HEAD_DIM)
        self.back[head, : spans - 1, 0] = (scale * self.acc[0]).astype(jnp.bfloat16).reshape(shape)
        self.back[head, : spans - 1, 1] = self.acc[1].astype(jnp.bfloat16).reshape(shape)

    def send_home(self, head):
        def send(to, carry):
            self.back_copy(head, to, self.me).start()
            return carry

        lax.fori_loop(0, self.me, send, 0)

    def attend_tile(self, head, step, carry):
        tile, spans, far_rows = self.tile, self.spans, self.far_rows
        scale = HEAD_DIM ** (-0.5)
        columns = slice(head * HEAD_DIM, (head + 1) * HEAD_DIM)
        rows = pl.ds(pl.multiple_of(step * tile, tile), tile)
        query = self.query[rows, columns]
        key = self.key[rows, columns]
        value = self.value[rows, columns]
        cot = self.cot[rows, columns]
        far_k = self.far[head, : spans - 1, 0].reshape(far_rows, HEAD_DIM)
        far_v = self.far[head, : spans - 1, 1].reshape(far_rows, HEAD_DIM)
        far_bias = self.bias[head, : (spans - 1) * CAP, rows]
        sums = self.bias[head, spans * CAP :, rows]
        far_bias = jnp.broadcast_to(
            far_bias[:, None, :], ((spans - 1) * CAP, KEY_BLOCK, tile)
        ).reshape(far_rows, tile)
        j = lax.broadcasted_iota(jnp.int32, (SUB, tile), 0)
        t = lax.broadcasted_iota(jnp.int32, (SUB, tile), 1) % SUB
        own_ok = (j // KEY_BLOCK == t // KEY_BLOCK) & (j <= t)
        own_bias = jnp.where(own_ok, 0.0, NEVER) + sums[0:1]

        parts = [slice(at, at + SUB) for at in range(0, tile, SUB)]
        own_s = jnp.concatenate([dot(key[r, :], query[r, :], NT) for r in parts], axis=1)
        own_g = jnp.concatenate([dot(value[r, :], cot[r, :], NT) for r in parts], axis=1)
        far_s = dot(far_k, query, NT)
        far_g = dot(far_v, cot, NT)
        far_p = jnp.exp2(far_s * (scale * LOG2E) + far_bias)
        own_p = jnp.exp2(own_s * (scale * LOG2E) + own_bias)
        row_dots = jnp.sum(far_p * far_g, axis=0, keepdims=True) + jnp.sum(
            own_p * own_g, axis=0, keepdims=True
        )
        far_d = (far_p * (far_g - row_dots)).astype(jnp.bfloat16)
        own_d = (own_p * (own_g - row_dots)).astype(jnp.bfloat16)
        far_low = far_p.astype(jnp.bfloat16)
        own_low = own_p.astype(jnp.bfloat16)

        turned = dot(self.key_turned[...], far_d, NN) + jnp.concatenate(
            [dot(key[r, :], own_d[:, r], TN) for r in parts], axis=1
        )
        self.dq[head, rows, :] = (scale * turned).T.astype(jnp.bfloat16)
        for r in parts:
            here = pl.ds(pl.multiple_of(step * tile + r.start, SUB), SUB)
            self.dkv[head, 0, here, :] = scale * dot(own_d[:, r], query[r, :], NN)
            self.dkv[head, 1, here, :] = dot(own_low[:, r], cot[r, :], NN)
        self.acc[0] += dot(far_d, query, NN)
        self.acc[1] += dot(far_low, cot, NN)
        self.dq_copy(head, step).start()
        return carry

    def source(self, kind, head):
        return (self.dq if kind == "own" else self.came)[head]

    def place_of(self, slot):
        left = self.pieces - 1 - slot
        place = self.me
        for bit in range(1, self.stages):
            on = lax.rem(lax.div(left, 2 ** (self.stages - 1 - bit)), 2)
            place = place + on * (flip(self.me, 2**bit) - self.me)
        return place

    def product(self, c):
        chunk = self.chunks[c]
        part = getattr(self, f"part{c}")
        give = getattr(self, f"give{c}_0")
        for kind, head in chunk:
            if kind == "came":

                def arrived(tile, carry, head=head):
                    self.dq_copy(head, tile).wait_recv()
                    return carry

                lax.fori_loop(0, self.tiles, arrived, 0)
        if c == 0:

            def turned(place, carry):
                self.turn_copy(place).wait_recv()
                return carry

            lax.fori_loop(0, self.spans, turned, 0)
        bit = lax.rem(self.me, 2)

        def one(slot, carry):
            pair = lax.div(self.place_of(slot), 2) * 2
            left = self.turned[pl.ds(pair, 2)].reshape(4 * self.slice, self.rows)
            right = jnp.concatenate([self.source(*s) for s in chunk], axis=1)
            part[slot] = dot(left, right, NN).reshape(part.shape[1:])
            give[slot] = part[slot, 1 - bit].astype(jnp.bfloat16)
            self.give_copy(c, 0, slot).start()
            return carry

        lax.fori_loop(0, self.pieces, one, 0)

    def ranges(self):
        low, out = 0, []
        for stage in range(1, self.stages):
            half = (self.pieces - low) // 2
            out.append((stage, low, half))
            low += half
        return out

    def total(self, c, slot):
        part = getattr(self, f"part{c}")
        self.give_copy(c, 0, slot).wait_recv()
        value = part[slot, lax.rem(self.me, 2)]
        value = value + getattr(self, f"got{c}_0")[slot].astype(jnp.float32)
        for stage, first, half in self.ranges():
            if slot < first + half:
                break
            at = slot - half - first
            self.give_copy(c, stage, at).wait_recv()
            value = value + getattr(self, f"got{c}_{stage}")[at].astype(jnp.float32)
        return value

    def relay(self, c, ranges):
        for stage, first, half in ranges:
            for slot in range(first, first + half):
                give = getattr(self, f"give{c}_{stage}")
                give[slot - first] = self.total(c, slot).astype(jnp.bfloat16)
                self.give_copy(c, stage, slot - first).start()

    def first(self, c):
        self.relay(c, self.ranges()[:1])

    def rest(self, c):
        self.relay(c, self.ranges()[1:])

    def settle(self, c):
        final = getattr(self, f"sum{c}")
        final[...] = self.total(c, self.pieces - 1).reshape(final.shape)
        self.sum_copy(c).start()
        for at, (kind, head) in enumerate(self.chunks[c]):
            self.put(self.tp, kind, head, final[0, :, at * HEAD_DIM : (at + 1) * HEAD_DIM])

    def put(self, tp, kind, head, block):
        if kind == "came":
            tp = flip(tp, self.side)
        column = pl.multiple_of((tp * self.heads + head) * HEAD_DIM, HEAD_DIM)
        self.weight[:, pl.ds(column, HEAD_DIM)] = block

    def finish(self):
        for c, chunk in enumerate(self.chunks):
            self.sum_copy(c).wait_recv()
            other = getattr(self, f"other{c}")
            for at, (kind, head) in enumerate(chunk):
                self.put(
                    flip(self.tp, 1), kind, head, other[:, at * HEAD_DIM : (at + 1) * HEAD_DIM]
                )
            self.sum_copy(c).wait_send()
            for stage in range(self.stages):
                for slot in range(getattr(self, f"give{c}_{stage}").shape[0]):
                    self.give_copy(c, stage, slot).wait_send()

        def turned(place, carry):
            self.turn_copy(place).wait_send()
            return carry

        lax.fori_loop(0, self.spans, turned, 0)
        for head in range(self.heads):

            def later(span, carry, head=head):
                self.far_copy(head, span, self.me).wait_send()
                self.back_copy(head, self.me, span).wait_recv()
                return carry

            lax.fori_loop(self.me + 1, self.spans, later, 0)

            def earlier(span, carry, head=head):
                self.back_copy(head, span, self.me).wait_send()
                return carry

            lax.fori_loop(0, self.me, earlier, 0)

            def sent(tile, carry, head=head):
                self.dq_copy(head, tile).wait_send()
                return carry

            lax.fori_loop(0, self.tiles, sent, 0)
            self.result_copy(head, 0).wait()
            self.result_copy(head, 1).wait()


def whole_step(chosen, sums, picked, query, key, value, cot, layer, tp_count):
    spans, heads = picked.shape[:2]
    rows = query.shape[0]
    plan = Kernel(spans, tp_count, heads, rows, layer.shape[1])
    scratch = plan.scratch()
    names = tuple(scratch)
    vmem = pl.BlockSpec(memory_space=pltpu.VMEM)
    hbm = pl.BlockSpec(memory_space=pl.ANY)
    wide = heads * HEAD_DIM
    return pl.pallas_call(
        functools.partial(plan.body, names),
        out_shape=(
            jax.ShapeDtypeStruct((rows, wide), jnp.bfloat16),
            jax.ShapeDtypeStruct((heads, 2, rows, HEAD_DIM), jnp.float32),
            jax.ShapeDtypeStruct((spans, heads, 2, CAP * KEY_BLOCK, HEAD_DIM), jnp.bfloat16),
            jax.ShapeDtypeStruct((plan.slice, tp_count * wide), jnp.float32),
        ),
        in_specs=[vmem] * 3 + [hbm] * 5,
        out_specs=(hbm, hbm, hbm, vmem),
        scratch_shapes=list(scratch.values()),
        compiler_params=pltpu.CompilerParams(
            collective_id=0, has_side_effects=True, vmem_limit_bytes=67043328
        ),
        name="whole_step",
    )(chosen, sums, picked, query, key, value, cot, layer)


def prepare_body(
    chosen, key_in, value_in, ids, picked, key, value, found, marks, sem, mark_sem
):
    loads = [
        pltpu.make_async_copy(src, dst, sem.at[i])
        for i, (src, dst) in enumerate(((key_in, key), (value_in, value)))
    ]
    for load in loads:
        load.start()
    spans, heads = picked.shape[:2]
    blocks = key.shape[0] // KEY_BLOCK
    count = chosen.shape[2]
    first = lax.axis_index("kv") * blocks
    asker = lax.broadcasted_iota(jnp.int32, (spans, count), 1) // blocks
    asks = asker == lax.broadcasted_iota(jnp.int32, (spans, count), 0)
    lane = lax.broadcasted_iota(jnp.int32, (spans, 128), 1)
    for head in range(heads):
        lists = chosen[head] - first
        mine = (lists >= 0) & (lists < blocks)
        low = jnp.min(jnp.where(mine, lists, blocks), axis=0, keepdims=True)
        high = jnp.max(jnp.where(mine, lists, 0), axis=0, keepdims=True)
        low = jnp.min(jnp.where(asks, low, blocks), axis=1, keepdims=True)
        high = jnp.max(jnp.where(asks, high, 0), axis=1, keepdims=True)
        low = jnp.where(low == blocks, 0, low)
        found[head] = jnp.where(lane == 0, low, high)
    copy = pltpu.make_async_copy(found, marks, mark_sem)
    copy.start()

    copy.wait()
    for load in loads:
        load.wait()

    def one(span, carry):
        for head in range(heads):
            columns = slice(head * HEAD_DIM, (head + 1) * HEAD_DIM)
            for slot in range(CAP):
                block = marks[head, span, slot]
                ids[slot, head * spans + span] = block
                at = pl.ds(pl.multiple_of(block * KEY_BLOCK, KEY_BLOCK), KEY_BLOCK)
                to = slice(slot * KEY_BLOCK, (slot + 1) * KEY_BLOCK)
                picked[span, head, 0, to, :] = key[at, columns]
                picked[span, head, 1, to, :] = value[at, columns]
        return carry

    lax.fori_loop(0, spans, one, 0)


def prepare(chosen, key, value, spans):
    heads = chosen.shape[0]
    vmem = pl.BlockSpec(memory_space=pltpu.VMEM)
    smem = pl.BlockSpec(memory_space=pltpu.SMEM)
    hbm = pl.BlockSpec(memory_space=pl.ANY)
    return pl.pallas_call(
        prepare_body,
        out_shape=(
            jax.ShapeDtypeStruct((CAP, heads * spans), jnp.int32),
            jax.ShapeDtypeStruct((spans, heads, 2, CAP * KEY_BLOCK, HEAD_DIM), jnp.bfloat16),
        ),
        in_specs=[vmem, hbm, hbm],
        out_specs=(smem, vmem),
        scratch_shapes=[
            pltpu.VMEM(key.shape, key.dtype),
            pltpu.VMEM(value.shape, value.dtype),
            pltpu.VMEM((heads, spans, 128), jnp.int32),
            pltpu.SMEM((heads, spans, 128), jnp.int32),
            pltpu.SemaphoreType.DMA((2,)),
            pltpu.SemaphoreType.DMA,
        ],
        name="prepare_blocks",
    )(chosen, key, value)


def land_body(
    ids, own_in, home_in, dq_in, weight_in, dq_out, out_k, out_v, weight_out,
    own, home, dq, weight, load_sem, store_sem,
):
    heads = own.shape[0]
    spans = home.shape[0]
    parts = [(head, kind) for head in range(heads) for kind in range(2)]
    loads, stores = [], []
    for head, kind in parts:
        columns = pl.ds(head * HEAD_DIM, HEAD_DIM)
        loads.append((own_in.at[head, kind], own.at[head, kind]))
        stores.append((own.at[head, kind], (out_k, out_v)[kind].at[:, columns]))
    loads += [(dq_in, dq), (weight_in, weight)]
    stores += [(dq, dq_out), (weight, weight_out)]
    first = pltpu.make_async_copy(home_in, home, load_sem.at[len(loads)])
    first.start()
    loads = [pltpu.make_async_copy(*pair, load_sem.at[i]) for i, pair in enumerate(loads)]
    stores = [pltpu.make_async_copy(*pair, store_sem.at[i]) for i, pair in enumerate(stores)]
    for load in loads:
        load.start()
    first.wait()
    for i, load in enumerate(loads):
        load.wait()
        if i < len(parts):
            head, kind = parts[i]

            def one(span, carry, head=head, kind=kind):
                for slot in range(CAP):
                    start = ids[slot, head * spans + span] * KEY_BLOCK
                    rows = pl.ds(pl.multiple_of(start, KEY_BLOCK), KEY_BLOCK)
                    at = slice(slot * KEY_BLOCK, (slot + 1) * KEY_BLOCK)
                    own[head, kind, rows, :] += home[span, head, kind, at, :].astype(jnp.float32)
                return carry

            lax.fori_loop(lax.axis_index("kv") + 1, spans, one, 0)
        stores[i].start()
    for store in stores:
        store.wait()


def land(ids, own, home, dq, weight):
    heads, _, rows, _ = own.shape
    smem = pl.BlockSpec(memory_space=pltpu.SMEM)
    hbm = pl.BlockSpec(memory_space=pl.ANY)
    whole = jax.ShapeDtypeStruct((rows, heads * HEAD_DIM), jnp.float32)
    like = [jax.ShapeDtypeStruct(x.shape, x.dtype) for x in (dq, weight)]
    return pl.pallas_call(
        land_body,
        out_shape=(like[0], whole, whole, like[1]),
        in_specs=[smem] + [hbm] * 4,
        out_specs=(hbm,) * 4,
        scratch_shapes=[pltpu.VMEM(x.shape, x.dtype) for x in (own, home, dq, weight)]
        + [pltpu.SemaphoreType.DMA((2 * heads + 3,)), pltpu.SemaphoreType.DMA((2 * heads + 2,))],
        name="land_blocks",
    )(ids, own, home, dq, weight)


def local(query_rows, key_rows, value_rows, log_sums, cotangent, layer_input, chosen):
    kv_count = lax.axis_size("kv")
    tp_count = lax.axis_size("tp")
    chosen = jnp.swapaxes(chosen, 1, 2)
    ids, picked = prepare(chosen, key_rows, value_rows, kv_count)
    dq, own, home, weight = whole_step(
        chosen, log_sums, picked, query_rows, key_rows, value_rows, cotangent, layer_input, tp_count
    )
    return land(ids, own, home, dq, weight)


def solution(mesh):
    placed = (
        P("kv", "tp"),
        P("kv", "tp"),
        P("kv", "tp"),
        P("tp", "kv"),
        P("kv", "tp"),
        P("kv", "tp"),
        P("tp", None, None),
    )
    return jax.shard_map(
        local,
        mesh=mesh,
        in_specs=placed,
        out_specs=(P("kv", "tp"), P("kv", "tp"), P("kv", "tp"), P(("tp", "kv"), None)),
        check_vma=False,
    )
```

```python
import functools

import jax
import jax.numpy as jnp
from jax import lax
from jax.experimental import pallas as pl
from jax.experimental.pallas import tpu as pltpu
from jax.sharding import PartitionSpec as P

HEAD_DIM = 128
KEY_BLOCK = 32
CAP = 2
SUB = 128
NEVER = -1e30
LOG2E = 1.4426950408889634

MESH = pl.DeviceIdType.MESH
NT = (((1,), (1,)), ((), ()))
NN = (((1,), (0,)), ((), ()))
TN = (((0,), (0,)), ((), ()))


def dot(a, b, dims):
    return lax.dot_general(a, b, dims, preferred_element_type=jnp.float32)


def flip(place, bit):
    return place + bit - 2 * bit * lax.rem(lax.div(place, bit), 2)


def chunk_plan(heads):
    own = [[("own", head)] for head in range(heads)]
    came = [[("came", head)] for head in range(heads)]
    return own[:1] + [own[1] + came[0]] + own[2:] + came[1:]


def step_plan(heads):
    plan = []
    for head in range(heads):
        plan += [("attend", head), ("product", head), ("send_home", head)]
        if head:
            plan.append(("first", head - 1))
    plan += [("rest", chunk) for chunk in range(heads - 2)]
    last = 2 * heads - 2
    for chunk in range(heads, last + 1):
        plan.append(("product", chunk))
        if chunk == heads:
            plan += [("first", heads - 1), ("rest", heads - 2)]
            plan += [("settle", early) for early in range(heads - 1)]
        else:
            plan.append(("settle", chunk - 2))
        plan += [("rest", chunk - 1), ("first", chunk)]
    return plan + [("settle", last - 1), ("rest", last), ("settle", last)]


class Kernel:
    def __init__(self, spans, tp_count, heads, rows, features):
        self.spans, self.tp_count, self.heads = spans, tp_count, heads
        self.rows, self.features = rows, features
        self.far_rows = (spans - 1) * CAP * KEY_BLOCK
        self.tile = 1024 if self.far_rows <= 512 else 128
        self.unit = min(self.tile, 512)
        self.units = rows // self.unit
        self.slice = features // spans
        self.pieces = spans // 2
        self.chunks = chunk_plan(heads)
        self.plan = step_plan(heads)
        self.stages = spans.bit_length() - 1

    def scratch(self):
        spans, heads, rows = self.spans, self.heads, self.rows
        span_rows = CAP * KEY_BLOCK
        wide = heads * HEAD_DIM
        bf, f32 = jnp.bfloat16, jnp.float32
        dma = pltpu.SemaphoreType.DMA
        out = dict(
            query=pltpu.VMEM((rows, wide), bf),
            key=pltpu.VMEM((rows, wide), bf),
            value=pltpu.VMEM((rows, wide), bf),
            cot=pltpu.VMEM((rows, wide), bf),
            layer=pltpu.VMEM((4, rows, HEAD_DIM), bf),
            layer_sem=dma((4,)),
            turned=pltpu.VMEM((spans, 2, self.slice, rows), bf),
            far=pltpu.VMEM((heads, spans, 2, span_rows, HEAD_DIM), bf),
            back=pltpu.VMEM((heads, spans, 2, span_rows, HEAD_DIM), bf),
            acc=pltpu.VMEM((2, self.far_rows, HEAD_DIM), f32),
            key_turned=pltpu.VMEM((HEAD_DIM, self.far_rows), bf),
            bias=pltpu.VMEM((heads, spans * CAP + 8, rows), f32),
            came=pltpu.VMEM((heads, rows, HEAD_DIM), bf),
            load_sem=dma((4,)),
            far_send=dma((heads, spans)),
            far_recv=dma((heads, spans)),
            back_send=dma((heads, spans)),
            back_recv=dma((heads, spans)),
            turn_send=dma((spans,)),
            turn_recv=dma((spans,)),
            dq_send=dma((heads, self.units)),
            dq_recv=dma((heads, self.units)),
        )
        count = len(self.chunks)
        for c, chunk in enumerate(self.chunks):
            width = HEAD_DIM * len(chunk)
            out[f"part{c}"] = pltpu.VMEM((self.pieces, 2, 2 * self.slice, width), f32)
            left = self.pieces
            for stage in range(self.stages):
                give = left if stage == 0 else left // 2
                shape = (give, 2 * self.slice, width)
                out[f"give{c}_{stage}"] = pltpu.VMEM(shape, bf)
                out[f"got{c}_{stage}"] = pltpu.VMEM(shape, bf)
                out[f"give_sem{c}_{stage}"] = dma((give,))
                out[f"got_sem{c}_{stage}"] = dma((give,))
                left = give if stage == 0 else left - give
            out[f"sum{c}"] = pltpu.VMEM((2, self.slice, width), f32)
            out[f"other{c}"] = pltpu.VMEM((self.slice, width), f32)
        out["sum_send"] = dma((count,))
        out["sum_recv"] = dma((count,))
        return out

    def body(self, names, *refs):
        fixed = (
            "chosen", "sums", "picked", "query_in", "key_in", "value_in", "cot_in", "layer_in", "dq", "own", "home", "weight",
        )
        for name, ref in zip(fixed + names, refs, strict=True):
            setattr(self, name, ref)
        self.me = lax.axis_index("kv")
        self.tp = lax.axis_index("tp")
        self.side = self.tp_count // 2
        self.start()
        for head in range(self.heads):
            self.send_far(head)
        self.turn()
        self.allow()
        for kind, index in self.plan:
            getattr(self, kind)(index)
        self.finish()


    def load(self, which):
        pairs = (
            (self.key_in, self.key),
            (self.value_in, self.value),
            (self.query_in, self.query),
            (self.cot_in, self.cot),
        )
        src, dst = pairs[which]
        return pltpu.make_async_copy(src, dst, self.load_sem.at[which])

    def layer_copy(self, group):
        columns = pl.ds(pl.multiple_of(group * HEAD_DIM, HEAD_DIM), HEAD_DIM)
        slot = lax.rem(group, 4)
        return pltpu.make_async_copy(
            self.layer_in.at[:, columns], self.layer.at[slot], self.layer_sem.at[slot]
        )

    def remote(self, src, dst, send, recv, **to):
        return pltpu.make_async_remote_copy(
            src_ref=src, dst_ref=dst, send_sem=send, recv_sem=recv,
            device_id=to, device_id_type=MESH,
        )

    def far_copy(self, head, to, sender):
        return self.remote(
            self.picked.at[to, head], self.far.at[head, sender],
            self.far_send.at[head, to], self.far_recv.at[head, sender], kv=to,
        )

    def back_copy(self, head, to, sender):
        return self.remote(
            self.back.at[head, to], self.home.at[sender, head],
            self.back_send.at[head, to], self.back_recv.at[head, sender], kv=to,
        )

    def turn_copy(self, place):
        return self.remote(
            self.turned.at[place, 0], self.turned.at[place, 1],
            self.turn_send.at[place], self.turn_recv.at[place], tp=flip(self.tp, 1),
        )

    def dq_copy(self, head, tile):
        rows = pl.ds(pl.multiple_of(tile * self.unit, self.unit), self.unit)
        return self.remote(
            self.dq.at[head, rows], self.came.at[head, rows],
            self.dq_send.at[head, tile], self.dq_recv.at[head, tile],
            tp=flip(self.tp, self.side),
        )

    def give_copy(self, c, stage, slot):
        return self.remote(
            getattr(self, f"give{c}_{stage}").at[slot],
            getattr(self, f"got{c}_{stage}").at[slot],
            getattr(self, f"give_sem{c}_{stage}").at[slot],
            getattr(self, f"got_sem{c}_{stage}").at[slot],
            kv=flip(self.me, 2**stage),
        )

    def sum_copy(self, c):
        return self.remote(
            getattr(self, f"sum{c}").at[1], getattr(self, f"other{c}"),
            self.sum_send.at[c], self.sum_recv.at[c], tp=flip(self.tp, 1),
        )


    def start(self):
        for which in range(4):
            self.load(which).start()
        for group in range(4):
            self.layer_copy(group).start()
        barrier = pltpu.get_barrier_semaphore()

        def greet(step, carry):
            to = lax.rem(self.me + step, self.spans)
            pl.semaphore_signal(barrier, inc=1, device_id={"kv": to}, device_id_type=MESH)
            return carry

        lax.fori_loop(1, self.spans, greet, 0)
        for bit in (1, self.side):
            pl.semaphore_signal(
                barrier, inc=1, device_id={"tp": flip(self.tp, bit)}, device_id_type=MESH
            )

        def blank(span, carry):
            for head in range(self.heads):
                self.far[head, span] = jnp.zeros(self.far.shape[2:], jnp.bfloat16)
            return carry

        lax.fori_loop(self.me, self.spans, blank, 0)
        pl.semaphore_wait(barrier, self.spans + 1)

    def send_far(self, head):
        def send(step, carry):
            self.far_copy(head, self.spans - 1 - step, self.me).start()
            return carry

        lax.fori_loop(0, self.spans - 1 - self.me, send, 0)

    def allow(self):
        spans, rows, heads = self.spans, self.rows, self.heads
        blocks = rows // KEY_BLOCK
        entries = self.chosen.shape[1]
        first = self.me * blocks
        group = lax.div(first, 128) * 128
        shift = first - group
        row = lax.broadcasted_iota(jnp.int32, (128, rows), 0) - shift
        of = lax.broadcasted_iota(jnp.int32, (128, rows), 1) // KEY_BLOCK
        spread = jnp.where(row == of, 1.0, 0.0).astype(jnp.bfloat16)
        wide = (spans * CAP, 128)
        slot = lax.broadcasted_iota(jnp.int32, wide, 0)
        base = slot // CAP * blocks
        lane = lax.broadcasted_iota(jnp.int32, (1, 128), 1)
        here = (lane >= shift) & (lane < shift + blocks)
        for head in range(heads):
            at = pl.ds(pl.multiple_of(group, 128), 128)
            own = [jnp.where(here, self.chosen[head, e : e + 1, at], -1) for e in range(entries)]
            low = jnp.full(wide, spans * blocks, jnp.int32)
            high = jnp.full(wide, -2, jnp.int32)
            for entry in own:
                inside = (entry >= base) & (entry < base + blocks)
                low = jnp.minimum(low, jnp.where(inside, entry, spans * blocks))
                high = jnp.maximum(high, jnp.where(inside, entry, -2))
            low = jnp.min(low, axis=1, keepdims=True)
            high = jnp.max(high, axis=1, keepdims=True)
            high = jnp.where(high == low, -2, high)
            wanted = jnp.where(slot % CAP == 0, low, high)
            hit = own[0] == wanted
            for entry in own[1:]:
                hit = hit | (entry == wanted)
            hits = jnp.where(hit, 1.0, 0.0).astype(jnp.bfloat16)
            used = dot(hits, spread, NN)
            minus = self.sums[head : head + 1, :] * -LOG2E
            self.bias[head, : spans * CAP, :] = jnp.where(used > 0.5, minus, NEVER)
            self.bias[head, spans * CAP :, :] = jnp.broadcast_to(minus, (8, rows))

    def turn(self):
        group = HEAD_DIM // self.slice
        step_rows = 512
        last = self.features // HEAD_DIM

        def one(g, carry):
            self.layer_copy(g).wait()
            for at in range(0, self.rows, step_rows):
                block = self.layer[lax.rem(g, 4), at : at + step_rows, :].T
                for j in range(group):
                    self.turned[g * group + j, 0, :, at : at + step_rows] = block[
                        j * self.slice : (j + 1) * self.slice
                    ]

            @pl.when(g + 4 < last)
            def _():
                self.layer_copy(g + 4).start()

            @pl.when(g > 0)
            def _():
                for j in range(group):
                    self.turn_copy((g - 1) * group + j).start()

            return carry

        lax.fori_loop(0, last, one, 0)
        for which in range(4):
            self.load(which).wait()
        for j in range(group):
            self.turn_copy((last - 1) * group + j).start()

    def attend(self, head):
        def arrived(span, carry):
            self.far_copy(head, self.me, span).wait_recv()
            return carry

        lax.fori_loop(0, self.me, arrived, 0)
        far_k = self.far[head, : self.spans - 1, 0].reshape(self.far_rows, HEAD_DIM)
        self.key_turned[...] = far_k.T
        self.acc[...] = jnp.zeros_like(self.acc)
        tile = self.tile if head else self.unit
        lax.fori_loop(
            0, self.rows // tile, functools.partial(self.attend_tile, head, tile), 0
        )
        scale = HEAD_DIM ** (-0.5)
        spans = self.spans
        shape = (spans - 1, CAP * KEY_BLOCK, HEAD_DIM)
        self.back[head, : spans - 1, 0] = (scale * self.acc[0]).astype(jnp.bfloat16).reshape(shape)
        self.back[head, : spans - 1, 1] = self.acc[1].astype(jnp.bfloat16).reshape(shape)

    def send_home(self, head):
        def send(to, carry):
            self.back_copy(head, to, self.me).start()
            return carry

        lax.fori_loop(0, self.me, send, 0)

    def attend_tile(self, head, tile, step, carry):
        spans, far_rows = self.spans, self.far_rows
        scale = HEAD_DIM ** (-0.5)
        columns = slice(head * HEAD_DIM, (head + 1) * HEAD_DIM)
        rows = pl.ds(pl.multiple_of(step * tile, tile), tile)
        query = self.query[rows, columns]
        key = self.key[rows, columns]
        value = self.value[rows, columns]
        cot = self.cot[rows, columns]
        far_k = self.far[head, : spans - 1, 0].reshape(far_rows, HEAD_DIM)
        far_v = self.far[head, : spans - 1, 1].reshape(far_rows, HEAD_DIM)
        far_bias = self.bias[head, : (spans - 1) * CAP, rows]
        sums = self.bias[head, spans * CAP :, rows]
        far_bias = jnp.broadcast_to(
            far_bias[:, None, :], ((spans - 1) * CAP, KEY_BLOCK, tile)
        ).reshape(far_rows, tile)
        j = lax.broadcasted_iota(jnp.int32, (SUB, tile), 0)
        t = lax.broadcasted_iota(jnp.int32, (SUB, tile), 1) % SUB
        own_ok = (j // KEY_BLOCK == t // KEY_BLOCK) & (j <= t)
        own_bias = jnp.where(own_ok, 0.0, NEVER) + sums[0:1]

        parts = [slice(at, at + SUB) for at in range(0, tile, SUB)]
        own_s = jnp.concatenate([dot(key[r, :], query[r, :], NT) for r in parts], axis=1)
        own_g = jnp.concatenate([dot(value[r, :], cot[r, :], NT) for r in parts], axis=1)
        far_s = dot(far_k, query, NT)
        far_g = dot(far_v, cot, NT)
        far_p = jnp.exp2(far_s * (scale * LOG2E) + far_bias)
        own_p = jnp.exp2(own_s * (scale * LOG2E) + own_bias)
        row_dots = jnp.sum(far_p * far_g, axis=0, keepdims=True) + jnp.sum(
            own_p * own_g, axis=0, keepdims=True
        )
        far_d = (far_p * (far_g - row_dots)).astype(jnp.bfloat16)
        own_d = (own_p * (own_g - row_dots)).astype(jnp.bfloat16)
        far_low = far_p.astype(jnp.bfloat16)
        own_low = own_p.astype(jnp.bfloat16)

        turned = dot(self.key_turned[...], far_d, NN) + jnp.concatenate(
            [dot(key[r, :], own_d[:, r], TN) for r in parts], axis=1
        )
        self.dq[head, rows, :] = (scale * turned).T.astype(jnp.bfloat16)
        for r in parts:
            here = pl.ds(pl.multiple_of(step * tile + r.start, SUB), SUB)
            self.own[head, 0, here, :] = scale * dot(own_d[:, r], query[r, :], NN)
            self.own[head, 1, here, :] = dot(own_low[:, r], cot[r, :], NN)
        self.acc[0] += dot(far_d, query, NN)
        self.acc[1] += dot(far_low, cot, NN)
        count = tile // self.unit
        for unit in range(count):
            self.dq_copy(head, step * count + unit).start()
        return carry

    def source(self, kind, head):
        return (self.dq if kind == "own" else self.came)[head]

    def place_of(self, slot):
        left = self.pieces - 1 - slot
        place = self.me
        for bit in range(1, self.stages):
            on = lax.rem(lax.div(left, 2 ** (self.stages - 1 - bit)), 2)
            place = place + on * (flip(self.me, 2**bit) - self.me)
        return place

    def product(self, c):
        chunk = self.chunks[c]
        part = getattr(self, f"part{c}")
        give = getattr(self, f"give{c}_0")
        for kind, head in chunk:
            if kind == "came":

                def arrived(tile, carry, head=head):
                    self.dq_copy(head, tile).wait_recv()
                    return carry

                lax.fori_loop(0, self.units, arrived, 0)
        if c == 0:

            def turned(place, carry):
                self.turn_copy(place).wait_recv()
                return carry

            lax.fori_loop(0, self.spans, turned, 0)
        bit = lax.rem(self.me, 2)

        def one(slot, carry):
            pair = lax.div(self.place_of(slot), 2) * 2
            left = self.turned[pl.ds(pair, 2)].reshape(4 * self.slice, self.rows)
            right = jnp.concatenate([self.source(*s) for s in chunk], axis=1)
            part[slot] = dot(left, right, NN).reshape(part.shape[1:])
            give[slot] = part[slot, 1 - bit].astype(jnp.bfloat16)
            self.give_copy(c, 0, slot).start()
            return carry

        lax.fori_loop(0, self.pieces, one, 0)

    def ranges(self):
        low, out = 0, []
        for stage in range(1, self.stages):
            half = (self.pieces - low) // 2
            out.append((stage, low, half))
            low += half
        return out

    def total(self, c, slot):
        part = getattr(self, f"part{c}")
        self.give_copy(c, 0, slot).wait_recv()
        value = part[slot, lax.rem(self.me, 2)]
        value = value + getattr(self, f"got{c}_0")[slot].astype(jnp.float32)
        for stage, first, half in self.ranges():
            if slot < first + half:
                break
            at = slot - half - first
            self.give_copy(c, stage, at).wait_recv()
            value = value + getattr(self, f"got{c}_{stage}")[at].astype(jnp.float32)
        return value

    def relay(self, c, ranges):
        for stage, first, half in ranges:
            for slot in range(first, first + half):
                give = getattr(self, f"give{c}_{stage}")
                give[slot - first] = self.total(c, slot).astype(jnp.bfloat16)
                self.give_copy(c, stage, slot - first).start()

    def first(self, c):
        self.relay(c, self.ranges()[:1])

    def rest(self, c):
        self.relay(c, self.ranges()[1:])

    def settle(self, c):
        final = getattr(self, f"sum{c}")
        final[...] = self.total(c, self.pieces - 1).reshape(final.shape)
        self.sum_copy(c).start()
        for at, (kind, head) in enumerate(self.chunks[c]):
            self.put(self.tp, kind, head, final[0, :, at * HEAD_DIM : (at + 1) * HEAD_DIM])

    def put(self, tp, kind, head, block):
        if kind == "came":
            tp = flip(tp, self.side)
        column = pl.multiple_of((tp * self.heads + head) * HEAD_DIM, HEAD_DIM)
        self.weight[:, pl.ds(column, HEAD_DIM)] = block

    def finish(self):
        for c, chunk in enumerate(self.chunks):
            self.sum_copy(c).wait_recv()
            other = getattr(self, f"other{c}")
            for at, (kind, head) in enumerate(chunk):
                self.put(
                    flip(self.tp, 1), kind, head, other[:, at * HEAD_DIM : (at + 1) * HEAD_DIM]
                )
            self.sum_copy(c).wait_send()
            for stage in range(self.stages):
                for slot in range(getattr(self, f"give{c}_{stage}").shape[0]):
                    self.give_copy(c, stage, slot).wait_send()

        def turned(place, carry):
            self.turn_copy(place).wait_send()
            return carry

        lax.fori_loop(0, self.spans, turned, 0)
        for head in range(self.heads):

            def later(span, carry, head=head):
                self.far_copy(head, span, self.me).wait_send()
                self.back_copy(head, self.me, span).wait_recv()
                return carry

            lax.fori_loop(self.me + 1, self.spans, later, 0)

            def earlier(span, carry, head=head):
                self.back_copy(head, span, self.me).wait_send()
                return carry

            lax.fori_loop(0, self.me, earlier, 0)

            def sent(tile, carry, head=head):
                self.dq_copy(head, tile).wait_send()
                return carry

            lax.fori_loop(0, self.units, sent, 0)


def whole_step(chosen, sums, picked, query, key, value, cot, layer, tp_count):
    spans, heads = picked.shape[:2]
    rows = query.shape[0]
    plan = Kernel(spans, tp_count, heads, rows, layer.shape[1])
    scratch = plan.scratch()
    names = tuple(scratch)
    vmem = pl.BlockSpec(memory_space=pltpu.VMEM)
    hbm = pl.BlockSpec(memory_space=pl.ANY)
    wide = heads * HEAD_DIM
    return pl.pallas_call(
        functools.partial(plan.body, names),
        out_shape=(
            pltpu.VMEM((heads, rows, HEAD_DIM), jnp.bfloat16),
            pltpu.VMEM((heads, 2, rows, HEAD_DIM), jnp.float32),
            pltpu.VMEM((spans, heads, 2, CAP * KEY_BLOCK, HEAD_DIM), jnp.bfloat16),
            pltpu.VMEM((plan.slice, tp_count * wide), jnp.float32),
        ),
        in_specs=[vmem] * 3 + [hbm] * 5,
        out_specs=(vmem,) * 4,
        scratch_shapes=list(scratch.values()),
        compiler_params=pltpu.CompilerParams(
            collective_id=0, has_side_effects=True, vmem_limit_bytes=50 * 2**20
        ),
        name="whole_step",
    )(chosen, sums, picked, query, key, value, cot, layer)


def prepare_body(
    chosen, key_in, value_in, ids, picked, key, value, found, marks, sem, mark_sem
):
    loads = [
        pltpu.make_async_copy(src, dst, sem.at[i])
        for i, (src, dst) in enumerate(((key_in, key), (value_in, value)))
    ]
    for load in loads:
        load.start()
    spans, heads = picked.shape[:2]
    blocks = key.shape[0] // KEY_BLOCK
    count = chosen.shape[2]
    first = lax.axis_index("kv") * blocks
    asker = lax.broadcasted_iota(jnp.int32, (spans, count), 1) // blocks
    asks = asker == lax.broadcasted_iota(jnp.int32, (spans, count), 0)
    lane = lax.broadcasted_iota(jnp.int32, (spans, 128), 1)
    for head in range(heads):
        lists = chosen[head] - first
        mine = (lists >= 0) & (lists < blocks)
        low = jnp.min(jnp.where(mine, lists, blocks), axis=0, keepdims=True)
        high = jnp.max(jnp.where(mine, lists, 0), axis=0, keepdims=True)
        low = jnp.min(jnp.where(asks, low, blocks), axis=1, keepdims=True)
        high = jnp.max(jnp.where(asks, high, 0), axis=1, keepdims=True)
        low = jnp.where(low == blocks, 0, low)
        found[head] = jnp.where(lane == 0, low, high)
    copy = pltpu.make_async_copy(found, marks, mark_sem)
    copy.start()

    copy.wait()
    for load in loads:
        load.wait()

    def one(span, carry):
        for head in range(heads):
            columns = slice(head * HEAD_DIM, (head + 1) * HEAD_DIM)
            for slot in range(CAP):
                block = marks[head, span, slot]
                ids[slot, head * spans + span] = block
                at = pl.ds(pl.multiple_of(block * KEY_BLOCK, KEY_BLOCK), KEY_BLOCK)
                to = slice(slot * KEY_BLOCK, (slot + 1) * KEY_BLOCK)
                picked[span, head, 0, to, :] = key[at, columns]
                picked[span, head, 1, to, :] = value[at, columns]
        return carry

    lax.fori_loop(0, spans, one, 0)


def prepare(chosen, key, value, spans):
    heads = chosen.shape[0]
    vmem = pl.BlockSpec(memory_space=pltpu.VMEM)
    smem = pl.BlockSpec(memory_space=pltpu.SMEM)
    hbm = pl.BlockSpec(memory_space=pl.ANY)
    return pl.pallas_call(
        prepare_body,
        out_shape=(
            jax.ShapeDtypeStruct((CAP, heads * spans), jnp.int32),
            pltpu.VMEM((spans, heads, 2, CAP * KEY_BLOCK, HEAD_DIM), jnp.bfloat16),
        ),
        in_specs=[vmem, hbm, hbm],
        out_specs=(smem, vmem),
        scratch_shapes=[
            pltpu.VMEM(key.shape, key.dtype),
            pltpu.VMEM(value.shape, value.dtype),
            pltpu.VMEM((heads, spans, 128), jnp.int32),
            pltpu.SMEM((heads, spans, 128), jnp.int32),
            pltpu.SemaphoreType.DMA((2,)),
            pltpu.SemaphoreType.DMA,
        ],
        name="prepare_blocks",
    )(chosen, key, value)


def land_body(ids, own, home, dq, weight, dq_out, out_k, out_v, weight_out, result, sem):
    heads = own.shape[0]
    spans = home.shape[0]
    stores = [(weight, weight_out)]
    for head in range(heads):
        columns = pl.ds(head * HEAD_DIM, HEAD_DIM)
        stores.append((dq.at[head], dq_out.at[:, columns]))
    for head in range(heads):
        columns = pl.ds(head * HEAD_DIM, HEAD_DIM)
        stores.append((result.at[head, 0], out_k.at[:, columns]))
        stores.append((result.at[head, 1], out_v.at[:, columns]))
    stores = [pltpu.make_async_copy(*pair, sem.at[i]) for i, pair in enumerate(stores)]
    ready = 1 + heads
    for store in stores[:ready]:
        store.start()
    for head in range(heads):
        for kind in range(2):
            result[head, kind] = own[head, kind]

            def one(span, carry, head=head, kind=kind):
                for slot in range(CAP):
                    start = ids[slot, head * spans + span] * KEY_BLOCK
                    rows = pl.ds(pl.multiple_of(start, KEY_BLOCK), KEY_BLOCK)
                    at = slice(slot * KEY_BLOCK, (slot + 1) * KEY_BLOCK)
                    add = home[span, head, kind, at, :].astype(jnp.float32)
                    result[head, kind, rows, :] += add
                return carry

            lax.fori_loop(lax.axis_index("kv") + 1, spans, one, 0)
            stores[ready + 2 * head + kind].start()
    for store in stores:
        store.wait()


def land(ids, own, home, dq, weight):
    heads, _, rows, _ = own.shape
    wide = heads * HEAD_DIM
    vmem = pl.BlockSpec(memory_space=pltpu.VMEM)
    hbm = pl.BlockSpec(memory_space=pl.ANY)
    whole = jax.ShapeDtypeStruct((rows, wide), jnp.float32)
    return pl.pallas_call(
        land_body,
        out_shape=(
            jax.ShapeDtypeStruct((rows, wide), dq.dtype),
            whole,
            whole,
            jax.ShapeDtypeStruct(weight.shape, weight.dtype),
        ),
        in_specs=[pl.BlockSpec(memory_space=pltpu.SMEM)] + [vmem] * 4,
        out_specs=(hbm,) * 4,
        scratch_shapes=[
            pltpu.VMEM(own.shape, own.dtype),
            pltpu.SemaphoreType.DMA((1 + 3 * heads,)),
        ],
        compiler_params=pltpu.CompilerParams(vmem_limit_bytes=16 * 2**20),
        name="land_blocks",
    )(ids, own, home, dq, weight)


def local(query_rows, key_rows, value_rows, log_sums, cotangent, layer_input, chosen):
    kv_count = lax.axis_size("kv")
    tp_count = lax.axis_size("tp")
    chosen = jnp.swapaxes(chosen, 1, 2)
    ids, picked = prepare(chosen, key_rows, value_rows, kv_count)
    picked = pltpu.with_memory_space_constraint(picked, pltpu.VMEM)
    dq, own, home, weight = whole_step(
        chosen, log_sums, picked, query_rows, key_rows, value_rows, cotangent, layer_input, tp_count
    )
    return land(ids, own, home, dq, weight)


def solution(mesh):
    placed = (
        P("kv", "tp"),
        P("kv", "tp"),
        P("kv", "tp"),
        P("tp", "kv"),
        P("kv", "tp"),
        P("kv", "tp"),
        P("tp", None, None),
    )
    return jax.shard_map(
        local,
        mesh=mesh,
        in_specs=placed,
        out_specs=(P("kv", "tp"), P("kv", "tp"), P("kv", "tp"), P(("tp", "kv"), None)),
        check_vma=False,
    )
```

```python
import functools

import jax
import jax.numpy as jnp
from jax import lax
from jax.experimental import pallas as pl
from jax.experimental.pallas import tpu as pltpu
from jax.sharding import PartitionSpec as P

HEAD_DIM = 128
KEY_BLOCK = 32
CAP = 2
SUB = 128
NEVER = -1e30
LOG2E = 1.4426950408889634

MESH = pl.DeviceIdType.MESH
NT = (((1,), (1,)), ((), ()))
NN = (((1,), (0,)), ((), ()))
TN = (((0,), (0,)), ((), ()))


def dot(a, b, dims):
    return lax.dot_general(a, b, dims, preferred_element_type=jnp.float32)


def flip(place, bit):
    return place + bit - 2 * bit * lax.rem(lax.div(place, bit), 2)


def chunk_plan(heads):
    own = [[("own", head)] for head in range(heads)]
    came = [[("came", head)] for head in range(heads)]
    return own[:1] + [own[1] + came[0]] + own[2:] + came[1:]


def step_plan(heads):
    plan = []
    for head in range(heads):
        plan += [("attend", head), ("product", head)]
        if head < heads - 1:
            plan.append(("send_home", head))
        if head:
            plan.append(("first", head - 1))
    plan += [("rest", chunk) for chunk in range(heads - 2)]
    last = 2 * heads - 2
    for chunk in range(heads, last + 1):
        plan.append(("product", chunk))
        if chunk == heads:
            plan.append(("send_home", heads - 1))
            plan += [("first", heads - 1), ("rest", heads - 2)]
            plan += [("settle", early) for early in range(heads - 1)]
        else:
            plan.append(("settle", chunk - 2))
        plan += [("rest", chunk - 1), ("first", chunk)]
    return plan + [("settle", last - 1), ("rest", last), ("settle", last)]


class Kernel:
    def __init__(self, spans, tp_count, heads, rows, features):
        self.spans, self.tp_count, self.heads = spans, tp_count, heads
        self.rows, self.features = rows, features
        self.far_rows = (spans - 1) * CAP * KEY_BLOCK
        self.tile = 1024 if self.far_rows <= 512 else 128
        self.unit = min(self.tile, 512)
        self.units = rows // self.unit
        self.slice = features // spans
        self.pieces = spans // 2
        self.chunks = chunk_plan(heads)
        self.plan = step_plan(heads)
        self.stages = spans.bit_length() - 1

    def scratch(self):
        spans, heads, rows = self.spans, self.heads, self.rows
        span_rows = CAP * KEY_BLOCK
        wide = heads * HEAD_DIM
        bf, f32 = jnp.bfloat16, jnp.float32
        dma = pltpu.SemaphoreType.DMA
        out = dict(
            query=pltpu.VMEM((rows, wide), bf),
            key=pltpu.VMEM((rows, wide), bf),
            value=pltpu.VMEM((rows, wide), bf),
            cot=pltpu.VMEM((rows, wide), bf),
            layer=pltpu.VMEM((4, rows, HEAD_DIM), bf),
            layer_sem=dma((4,)),
            turned=pltpu.VMEM((spans, 2, self.slice, rows), bf),
            far=pltpu.VMEM((heads, spans, 2, span_rows, HEAD_DIM), bf),
            back=pltpu.VMEM((heads, spans, 2, span_rows, HEAD_DIM), bf),
            acc=pltpu.VMEM((2, self.far_rows, HEAD_DIM), f32),
            key_turned=pltpu.VMEM((HEAD_DIM, self.far_rows), bf),
            bias=pltpu.VMEM((heads, spans * CAP + 8, rows), f32),
            came=pltpu.VMEM((heads, rows, HEAD_DIM), bf),
            load_sem=dma((4,)),
            far_send=dma((heads, spans)),
            far_recv=dma((heads, spans)),
            back_send=dma((heads, spans)),
            back_recv=dma((heads, spans)),
            turn_send=dma((spans,)),
            turn_recv=dma((spans,)),
            dq_send=dma((heads, self.units)),
            dq_recv=dma((heads, self.units)),
        )
        count = len(self.chunks)
        for c, chunk in enumerate(self.chunks):
            width = HEAD_DIM * len(chunk)
            out[f"part{c}"] = pltpu.VMEM((self.pieces, 2, 2 * self.slice, width), f32)
            left = self.pieces
            for stage in range(self.stages):
                give = left if stage == 0 else left // 2
                shape = (give, 2 * self.slice, width)
                out[f"give{c}_{stage}"] = pltpu.VMEM(shape, bf)
                out[f"got{c}_{stage}"] = pltpu.VMEM(shape, bf)
                out[f"give_sem{c}_{stage}"] = dma((give,))
                out[f"got_sem{c}_{stage}"] = dma((give,))
                left = give if stage == 0 else left - give
            out[f"sum{c}"] = pltpu.VMEM((2, self.slice, width), f32)
            out[f"other{c}"] = pltpu.VMEM((self.slice, width), f32)
        out["sum_send"] = dma((count,))
        out["sum_recv"] = dma((count,))
        return out

    def body(self, names, *refs):
        fixed = (
            "chosen", "sums", "picked", "query_in", "key_in", "value_in", "cot_in", "layer_in", "dq", "own", "home", "weight",
        )
        for name, ref in zip(fixed + names, refs, strict=True):
            setattr(self, name, ref)
        self.me = lax.axis_index("kv")
        self.tp = lax.axis_index("tp")
        self.side = self.tp_count // 2
        self.start()
        for head in range(self.heads):
            self.send_far(head)
        self.turn()
        self.allow()
        for kind, index in self.plan:
            getattr(self, kind)(index)
        self.finish()


    def load(self, which):
        pairs = (
            (self.key_in, self.key),
            (self.value_in, self.value),
            (self.query_in, self.query),
            (self.cot_in, self.cot),
        )
        src, dst = pairs[which]
        return pltpu.make_async_copy(src, dst, self.load_sem.at[which])

    def layer_copy(self, group):
        columns = pl.ds(pl.multiple_of(group * HEAD_DIM, HEAD_DIM), HEAD_DIM)
        slot = lax.rem(group, 4)
        return pltpu.make_async_copy(
            self.layer_in.at[:, columns], self.layer.at[slot], self.layer_sem.at[slot]
        )

    def remote(self, src, dst, send, recv, **to):
        return pltpu.make_async_remote_copy(
            src_ref=src, dst_ref=dst, send_sem=send, recv_sem=recv,
            device_id=to, device_id_type=MESH,
        )

    def far_copy(self, head, to, sender):
        return self.remote(
            self.picked.at[to, head], self.far.at[head, sender],
            self.far_send.at[head, to], self.far_recv.at[head, sender], kv=to,
        )

    def back_copy(self, head, to, sender):
        return self.remote(
            self.back.at[head, to], self.home.at[sender, head],
            self.back_send.at[head, to], self.back_recv.at[head, sender], kv=to,
        )

    def turn_copy(self, place):
        return self.remote(
            self.turned.at[place, 0], self.turned.at[place, 1],
            self.turn_send.at[place], self.turn_recv.at[place], tp=flip(self.tp, 1),
        )

    def dq_copy(self, head, tile):
        rows = pl.ds(pl.multiple_of(tile * self.unit, self.unit), self.unit)
        return self.remote(
            self.dq.at[head, rows], self.came.at[head, rows],
            self.dq_send.at[head, tile], self.dq_recv.at[head, tile],
            tp=flip(self.tp, self.side),
        )

    def give_copy(self, c, stage, slot):
        return self.remote(
            getattr(self, f"give{c}_{stage}").at[slot],
            getattr(self, f"got{c}_{stage}").at[slot],
            getattr(self, f"give_sem{c}_{stage}").at[slot],
            getattr(self, f"got_sem{c}_{stage}").at[slot],
            kv=flip(self.me, 2**stage),
        )

    def sum_copy(self, c):
        return self.remote(
            getattr(self, f"sum{c}").at[1], getattr(self, f"other{c}"),
            self.sum_send.at[c], self.sum_recv.at[c], tp=flip(self.tp, 1),
        )


    def start(self):
        for which in range(4):
            self.load(which).start()
        for group in range(4):
            self.layer_copy(group).start()
        barrier = pltpu.get_barrier_semaphore()

        def greet(step, carry):
            to = lax.rem(self.me + step, self.spans)
            pl.semaphore_signal(barrier, inc=1, device_id={"kv": to}, device_id_type=MESH)
            return carry

        lax.fori_loop(1, self.spans, greet, 0)
        for bit in (1, self.side):
            pl.semaphore_signal(
                barrier, inc=1, device_id={"tp": flip(self.tp, bit)}, device_id_type=MESH
            )

        def blank(span, carry):
            for head in range(self.heads):
                self.far[head, span] = jnp.zeros(self.far.shape[2:], jnp.bfloat16)
            return carry

        lax.fori_loop(self.me, self.spans, blank, 0)
        pl.semaphore_wait(barrier, self.spans + 1)

    def send_far(self, head):
        def send(step, carry):
            self.far_copy(head, self.spans - 1 - step, self.me).start()
            return carry

        lax.fori_loop(0, self.spans - 1 - self.me, send, 0)

    def allow(self):
        spans, rows, heads = self.spans, self.rows, self.heads
        blocks = rows // KEY_BLOCK
        entries = self.chosen.shape[1]
        first = self.me * blocks
        group = lax.div(first, 128) * 128
        shift = first - group
        row = lax.broadcasted_iota(jnp.int32, (128, rows), 0) - shift
        of = lax.broadcasted_iota(jnp.int32, (128, rows), 1) // KEY_BLOCK
        spread = jnp.where(row == of, 1.0, 0.0).astype(jnp.bfloat16)
        wide = (spans * CAP, 128)
        slot = lax.broadcasted_iota(jnp.int32, wide, 0)
        base = slot // CAP * blocks
        lane = lax.broadcasted_iota(jnp.int32, (1, 128), 1)
        here = (lane >= shift) & (lane < shift + blocks)
        for head in range(heads):
            at = pl.ds(pl.multiple_of(group, 128), 128)
            own = [jnp.where(here, self.chosen[head, e : e + 1, at], -1) for e in range(entries)]
            low = jnp.full(wide, spans * blocks, jnp.int32)
            high = jnp.full(wide, -2, jnp.int32)
            for entry in own:
                inside = (entry >= base) & (entry < base + blocks)
                low = jnp.minimum(low, jnp.where(inside, entry, spans * blocks))
                high = jnp.maximum(high, jnp.where(inside, entry, -2))
            low = jnp.min(low, axis=1, keepdims=True)
            high = jnp.max(high, axis=1, keepdims=True)
            high = jnp.where(high == low, -2, high)
            wanted = jnp.where(slot % CAP == 0, low, high)
            hit = own[0] == wanted
            for entry in own[1:]:
                hit = hit | (entry == wanted)
            hits = jnp.where(hit, 1.0, 0.0).astype(jnp.bfloat16)
            used = dot(hits, spread, NN)
            minus = self.sums[head : head + 1, :] * -LOG2E
            self.bias[head, : spans * CAP, :] = jnp.where(used > 0.5, minus, NEVER)
            self.bias[head, spans * CAP :, :] = jnp.broadcast_to(minus, (8, rows))

    def turn(self):
        group = HEAD_DIM // self.slice
        step_rows = 512
        last = self.features // HEAD_DIM

        def one(g, carry):
            self.layer_copy(g).wait()
            for at in range(0, self.rows, step_rows):
                block = self.layer[lax.rem(g, 4), at : at + step_rows, :].T
                for j in range(group):
                    self.turned[g * group + j, 0, :, at : at + step_rows] = block[
                        j * self.slice : (j + 1) * self.slice
                    ]

            @pl.when(g + 4 < last)
            def _():
                self.layer_copy(g + 4).start()

            @pl.when(g > 0)
            def _():
                for j in range(group):
                    self.turn_copy((g - 1) * group + j).start()

            return carry

        lax.fori_loop(0, last, one, 0)
        for which in range(4):
            self.load(which).wait()
        for j in range(group):
            self.turn_copy((last - 1) * group + j).start()

    def attend(self, head):
        def arrived(span, carry):
            self.far_copy(head, self.me, span).wait_recv()
            return carry

        lax.fori_loop(0, self.me, arrived, 0)
        far_k = self.far[head, : self.spans - 1, 0].reshape(self.far_rows, HEAD_DIM)
        self.key_turned[...] = far_k.T
        self.acc[...] = jnp.zeros_like(self.acc)
        tile = self.tile if head else self.unit
        lax.fori_loop(
            0, self.rows // tile, functools.partial(self.attend_tile, head, tile), 0
        )
        scale = HEAD_DIM ** (-0.5)
        spans = self.spans
        shape = (spans - 1, CAP * KEY_BLOCK, HEAD_DIM)
        self.back[head, : spans - 1, 0] = (scale * self.acc[0]).astype(jnp.bfloat16).reshape(shape)
        self.back[head, : spans - 1, 1] = self.acc[1].astype(jnp.bfloat16).reshape(shape)

    def send_home(self, head):
        def send(to, carry):
            self.back_copy(head, to, self.me).start()
            return carry

        lax.fori_loop(0, self.me, send, 0)

    def attend_tile(self, head, tile, step, carry):
        spans, far_rows = self.spans, self.far_rows
        scale = HEAD_DIM ** (-0.5)
        columns = slice(head * HEAD_DIM, (head + 1) * HEAD_DIM)
        rows = pl.ds(pl.multiple_of(step * tile, tile), tile)
        query = self.query[rows, columns]
        key = self.key[rows, columns]
        value = self.value[rows, columns]
        cot = self.cot[rows, columns]
        far_k = self.far[head, : spans - 1, 0].reshape(far_rows, HEAD_DIM)
        far_v = self.far[head, : spans - 1, 1].reshape(far_rows, HEAD_DIM)
        far_bias = self.bias[head, : (spans - 1) * CAP, rows]
        sums = self.bias[head, spans * CAP :, rows]
        far_bias = jnp.broadcast_to(
            far_bias[:, None, :], ((spans - 1) * CAP, KEY_BLOCK, tile)
        ).reshape(far_rows, tile)
        j = lax.broadcasted_iota(jnp.int32, (SUB, tile), 0)
        t = lax.broadcasted_iota(jnp.int32, (SUB, tile), 1) % SUB
        own_ok = (j // KEY_BLOCK == t // KEY_BLOCK) & (j <= t)
        own_bias = jnp.where(own_ok, 0.0, NEVER) + sums[0:1]

        parts = [slice(at, at + SUB) for at in range(0, tile, SUB)]
        own_s = jnp.concatenate([dot(key[r, :], query[r, :], NT) for r in parts], axis=1)
        own_g = jnp.concatenate([dot(value[r, :], cot[r, :], NT) for r in parts], axis=1)
        far_s = dot(far_k, query, NT)
        far_g = dot(far_v, cot, NT)
        far_p = jnp.exp2(far_s * (scale * LOG2E) + far_bias)
        own_p = jnp.exp2(own_s * (scale * LOG2E) + own_bias)
        row_dots = jnp.sum(far_p * far_g, axis=0, keepdims=True) + jnp.sum(
            own_p * own_g, axis=0, keepdims=True
        )
        far_d = (far_p * (far_g - row_dots)).astype(jnp.bfloat16)
        own_d = (own_p * (own_g - row_dots)).astype(jnp.bfloat16)
        far_low = far_p.astype(jnp.bfloat16)
        own_low = own_p.astype(jnp.bfloat16)

        turned = dot(self.key_turned[...], far_d, NN) + jnp.concatenate(
            [dot(key[r, :], own_d[:, r], TN) for r in parts], axis=1
        )
        self.dq[head, rows, :] = (scale * turned).T.astype(jnp.bfloat16)
        for r in parts:
            here = pl.ds(pl.multiple_of(step * tile + r.start, SUB), SUB)
            self.own[head, 0, here, :] = scale * dot(own_d[:, r], query[r, :], NN)
            self.own[head, 1, here, :] = dot(own_low[:, r], cot[r, :], NN)
        self.acc[0] += dot(far_d, query, NN)
        self.acc[1] += dot(far_low, cot, NN)
        count = tile // self.unit
        for unit in range(count):
            self.dq_copy(head, step * count + unit).start()
        return carry

    def source(self, kind, head):
        return (self.dq if kind == "own" else self.came)[head]

    def place_of(self, slot):
        left = self.pieces - 1 - slot
        place = self.me
        for bit in range(1, self.stages):
            on = lax.rem(lax.div(left, 2 ** (self.stages - 1 - bit)), 2)
            place = place + on * (flip(self.me, 2**bit) - self.me)
        return place

    def product(self, c):
        chunk = self.chunks[c]
        part = getattr(self, f"part{c}")
        give = getattr(self, f"give{c}_0")
        for kind, head in chunk:
            if kind == "came":

                def arrived(tile, carry, head=head):
                    self.dq_copy(head, tile).wait_recv()
                    return carry

                lax.fori_loop(0, self.units, arrived, 0)
        if c == 0:

            def turned(place, carry):
                self.turn_copy(place).wait_recv()
                return carry

            lax.fori_loop(0, self.spans, turned, 0)
        bit = lax.rem(self.me, 2)

        def one(slot, carry):
            pair = lax.div(self.place_of(slot), 2) * 2
            left = self.turned[pl.ds(pair, 2)].reshape(4 * self.slice, self.rows)
            right = jnp.concatenate([self.source(*s) for s in chunk], axis=1)
            part[slot] = dot(left, right, NN).reshape(part.shape[1:])
            give[slot] = part[slot, 1 - bit].astype(jnp.bfloat16)
            self.give_copy(c, 0, slot).start()
            return carry

        lax.fori_loop(0, self.pieces, one, 0)

    def ranges(self):
        low, out = 0, []
        for stage in range(1, self.stages):
            half = (self.pieces - low) // 2
            out.append((stage, low, half))
            low += half
        return out

    def total(self, c, slot):
        part = getattr(self, f"part{c}")
        self.give_copy(c, 0, slot).wait_recv()
        value = part[slot, lax.rem(self.me, 2)]
        value = value + getattr(self, f"got{c}_0")[slot].astype(jnp.float32)
        for stage, first, half in self.ranges():
            if slot < first + half:
                break
            at = slot - half - first
            self.give_copy(c, stage, at).wait_recv()
            value = value + getattr(self, f"got{c}_{stage}")[at].astype(jnp.float32)
        return value

    def relay(self, c, ranges):
        for stage, first, half in ranges:
            for slot in range(first, first + half):
                give = getattr(self, f"give{c}_{stage}")
                give[slot - first] = self.total(c, slot).astype(jnp.bfloat16)
                self.give_copy(c, stage, slot - first).start()

    def first(self, c):
        self.relay(c, self.ranges()[:1])

    def rest(self, c):
        self.relay(c, self.ranges()[1:])

    def settle(self, c):
        final = getattr(self, f"sum{c}")
        final[...] = self.total(c, self.pieces - 1).reshape(final.shape)
        self.sum_copy(c).start()
        for at, (kind, head) in enumerate(self.chunks[c]):
            self.put(self.tp, kind, head, final[0, :, at * HEAD_DIM : (at + 1) * HEAD_DIM])

    def put(self, tp, kind, head, block):
        if kind == "came":
            tp = flip(tp, self.side)
        column = pl.multiple_of((tp * self.heads + head) * HEAD_DIM, HEAD_DIM)
        self.weight[:, pl.ds(column, HEAD_DIM)] = block

    def finish(self):
        for c, chunk in enumerate(self.chunks):
            self.sum_copy(c).wait_recv()
            other = getattr(self, f"other{c}")
            for at, (kind, head) in enumerate(chunk):
                self.put(
                    flip(self.tp, 1), kind, head, other[:, at * HEAD_DIM : (at + 1) * HEAD_DIM]
                )
            self.sum_copy(c).wait_send()
            for stage in range(self.stages):
                for slot in range(getattr(self, f"give{c}_{stage}").shape[0]):
                    self.give_copy(c, stage, slot).wait_send()

        def turned(place, carry):
            self.turn_copy(place).wait_send()
            return carry

        lax.fori_loop(0, self.spans, turned, 0)
        for head in range(self.heads):

            def later(span, carry, head=head):
                self.far_copy(head, span, self.me).wait_send()
                self.back_copy(head, self.me, span).wait_recv()
                return carry

            lax.fori_loop(self.me + 1, self.spans, later, 0)

            def earlier(span, carry, head=head):
                self.back_copy(head, span, self.me).wait_send()
                return carry

            lax.fori_loop(0, self.me, earlier, 0)

            def sent(tile, carry, head=head):
                self.dq_copy(head, tile).wait_send()
                return carry

            lax.fori_loop(0, self.units, sent, 0)


def whole_step(chosen, sums, picked, query, key, value, cot, layer, tp_count):
    spans, heads = picked.shape[:2]
    rows = query.shape[0]
    plan = Kernel(spans, tp_count, heads, rows, layer.shape[1])
    scratch = plan.scratch()
    names = tuple(scratch)
    vmem = pl.BlockSpec(memory_space=pltpu.VMEM)
    hbm = pl.BlockSpec(memory_space=pl.ANY)
    wide = heads * HEAD_DIM
    return pl.pallas_call(
        functools.partial(plan.body, names),
        out_shape=(
            pltpu.VMEM((heads, rows, HEAD_DIM), jnp.bfloat16),
            pltpu.VMEM((heads, 2, rows, HEAD_DIM), jnp.float32),
            pltpu.VMEM((spans, heads, 2, CAP * KEY_BLOCK, HEAD_DIM), jnp.bfloat16),
            pltpu.VMEM((plan.slice, tp_count * wide), jnp.float32),
        ),
        in_specs=[vmem] * 3 + [hbm] * 5,
        out_specs=(vmem,) * 4,
        scratch_shapes=list(scratch.values()),
        compiler_params=pltpu.CompilerParams(
            collective_id=0, has_side_effects=True, vmem_limit_bytes=50 * 2**20
        ),
        name="whole_step",
    )(chosen, sums, picked, query, key, value, cot, layer)


def prepare_body(
    chosen, key_in, value_in, ids, picked, key, value, found, marks, sem, mark_sem
):
    loads = [
        pltpu.make_async_copy(src, dst, sem.at[i])
        for i, (src, dst) in enumerate(((key_in, key), (value_in, value)))
    ]
    for load in loads:
        load.start()
    spans, heads = picked.shape[:2]
    blocks = key.shape[0] // KEY_BLOCK
    count = chosen.shape[2]
    first = lax.axis_index("kv") * blocks
    asker = lax.broadcasted_iota(jnp.int32, (spans, count), 1) // blocks
    asks = asker == lax.broadcasted_iota(jnp.int32, (spans, count), 0)
    lane = lax.broadcasted_iota(jnp.int32, (spans, 128), 1)
    for head in range(heads):
        lists = chosen[head] - first
        mine = (lists >= 0) & (lists < blocks)
        low = jnp.min(jnp.where(mine, lists, blocks), axis=0, keepdims=True)
        high = jnp.max(jnp.where(mine, lists, 0), axis=0, keepdims=True)
        low = jnp.min(jnp.where(asks, low, blocks), axis=1, keepdims=True)
        high = jnp.max(jnp.where(asks, high, 0), axis=1, keepdims=True)
        low = jnp.where(low == blocks, 0, low)
        found[head] = jnp.where(lane == 0, low, high)
    copy = pltpu.make_async_copy(found, marks, mark_sem)
    copy.start()

    copy.wait()
    for load in loads:
        load.wait()

    def one(span, carry):
        for head in range(heads):
            columns = slice(head * HEAD_DIM, (head + 1) * HEAD_DIM)
            for slot in range(CAP):
                block = marks[head, span, slot]
                ids[slot, head * spans + span] = block
                at = pl.ds(pl.multiple_of(block * KEY_BLOCK, KEY_BLOCK), KEY_BLOCK)
                to = slice(slot * KEY_BLOCK, (slot + 1) * KEY_BLOCK)
                picked[span, head, 0, to, :] = key[at, columns]
                picked[span, head, 1, to, :] = value[at, columns]
        return carry

    lax.fori_loop(0, spans, one, 0)


def prepare(chosen, key, value, spans):
    heads = chosen.shape[0]
    vmem = pl.BlockSpec(memory_space=pltpu.VMEM)
    smem = pl.BlockSpec(memory_space=pltpu.SMEM)
    hbm = pl.BlockSpec(memory_space=pl.ANY)
    return pl.pallas_call(
        prepare_body,
        out_shape=(
            jax.ShapeDtypeStruct((CAP, heads * spans), jnp.int32),
            pltpu.VMEM((spans, heads, 2, CAP * KEY_BLOCK, HEAD_DIM), jnp.bfloat16),
        ),
        in_specs=[vmem, hbm, hbm],
        out_specs=(smem, vmem),
        scratch_shapes=[
            pltpu.VMEM(key.shape, key.dtype),
            pltpu.VMEM(value.shape, value.dtype),
            pltpu.VMEM((heads, spans, 128), jnp.int32),
            pltpu.SMEM((heads, spans, 128), jnp.int32),
            pltpu.SemaphoreType.DMA((2,)),
            pltpu.SemaphoreType.DMA,
        ],
        name="prepare_blocks",
    )(chosen, key, value)


def land_body(ids, own, home, dq, weight, dq_out, out_k, out_v, weight_out, result, sem):
    heads = own.shape[0]
    spans = home.shape[0]
    stores = [(weight, weight_out)]
    for head in range(heads):
        columns = pl.ds(head * HEAD_DIM, HEAD_DIM)
        stores.append((dq.at[head], dq_out.at[:, columns]))
    for head in range(heads):
        columns = pl.ds(head * HEAD_DIM, HEAD_DIM)
        stores.append((result.at[head, 0], out_k.at[:, columns]))
        stores.append((result.at[head, 1], out_v.at[:, columns]))
    stores = [pltpu.make_async_copy(*pair, sem.at[i]) for i, pair in enumerate(stores)]
    ready = 1 + heads
    for store in stores[:ready]:
        store.start()
    for head in range(heads):
        for kind in range(2):
            result[head, kind] = own[head, kind]

            def one(span, carry, head=head, kind=kind):
                for slot in range(CAP):
                    start = ids[slot, head * spans + span] * KEY_BLOCK
                    rows = pl.ds(pl.multiple_of(start, KEY_BLOCK), KEY_BLOCK)
                    at = slice(slot * KEY_BLOCK, (slot + 1) * KEY_BLOCK)
                    add = home[span, head, kind, at, :].astype(jnp.float32)
                    result[head, kind, rows, :] += add
                return carry

            lax.fori_loop(lax.axis_index("kv") + 1, spans, one, 0)
            stores[ready + 2 * head + kind].start()
    for store in stores:
        store.wait()


def land(ids, own, home, dq, weight):
    heads, _, rows, _ = own.shape
    wide = heads * HEAD_DIM
    vmem = pl.BlockSpec(memory_space=pltpu.VMEM)
    hbm = pl.BlockSpec(memory_space=pl.ANY)
    whole = jax.ShapeDtypeStruct((rows, wide), jnp.float32)
    return pl.pallas_call(
        land_body,
        out_shape=(
            jax.ShapeDtypeStruct((rows, wide), dq.dtype),
            whole,
            whole,
            jax.ShapeDtypeStruct(weight.shape, weight.dtype),
        ),
        in_specs=[pl.BlockSpec(memory_space=pltpu.SMEM)] + [vmem] * 4,
        out_specs=(hbm,) * 4,
        scratch_shapes=[
            pltpu.VMEM(own.shape, own.dtype),
            pltpu.SemaphoreType.DMA((1 + 3 * heads,)),
        ],
        compiler_params=pltpu.CompilerParams(vmem_limit_bytes=16 * 2**20),
        name="land_blocks",
    )(ids, own, home, dq, weight)


def local(query_rows, key_rows, value_rows, log_sums, cotangent, layer_input, chosen):
    kv_count = lax.axis_size("kv")
    tp_count = lax.axis_size("tp")
    chosen = jnp.swapaxes(chosen, 1, 2)
    ids, picked = prepare(chosen, key_rows, value_rows, kv_count)
    picked = pltpu.with_memory_space_constraint(picked, pltpu.VMEM)
    dq, own, home, weight = whole_step(
        chosen, log_sums, picked, query_rows, key_rows, value_rows, cotangent, layer_input, tp_count
    )
    return land(ids, own, home, dq, weight)


def solution(mesh):
    placed = (
        P("kv", "tp"),
        P("kv", "tp"),
        P("kv", "tp"),
        P("tp", "kv"),
        P("kv", "tp"),
        P("kv", "tp"),
        P("tp", None, None),
    )
    return jax.shard_map(
        local,
        mesh=mesh,
        in_specs=placed,
        out_specs=(P("kv", "tp"), P("kv", "tp"), P("kv", "tp"), P(("tp", "kv"), None)),
        check_vma=False,
    )
```
